256 devices in a mesh: ep: 64 (over z, y, core), tp: 4 (over x).
Axes of the slice: x: 4, y: 4, z: 8, core: 2. Of those that a mesh axis runs over, the one named last changes fastest.
Arguments:
- tokens: bfloat16 [1024, 4096], P(None, 'ep'), may hold values from -80 to 80
- mix_gain: bfloat16 [4096], P('ep'), may hold values from 0.099609375 to 1.8984375
- w_query: bfloat16 [4096, 1024], P('ep', 'tp'), may hold values from -0.09375 to 0.09375
- w_key: bfloat16 [4096, 1024], P('ep', 'tp'), may hold values from -0.09375 to 0.09375
- w_value: bfloat16 [4096, 2048], P('ep', 'tp'), may hold values from -0.09375 to 0.09375
- w_outgate: bfloat16 [4096, 2048], P('ep', 'tp'), may hold values from -0.09375 to 0.09375
- w_igate: bfloat16 [4096, 16], P('ep', 'tp'), may hold values from -0.09375 to 0.09375
- w_fgate: bfloat16 [4096, 16], P('ep', 'tp'), may hold values from -0.09375 to 0.09375
- igate_bias: float32 [16], P('tp'), may hold values from -3 to 3
- fgate_bias: float32 [16], P('tp'), may hold values from -1 to 3
- head_gain: bfloat16 [2048], P('tp'), may hold values from 0.099609375 to 1.8984375
- w_mixout: bfloat16 [2048, 4096], P('tp', 'ep'), may hold values from -0.125 to 0.125
- state_matrix: float32 [1024, 16, 64, 128], P('ep', 'tp'), may hold values from -3 to 3
- state_norm: float32 [1024, 16, 64], P('ep', 'tp'), may hold values from -3 to 3
- state_max: float32 [1024, 16], P('ep', 'tp'), may hold values from -3 to 3
- ffn_gain: bfloat16 [4096], P('ep'), may hold values from 0.099609375 to 1.8984375
- dense_mix: bfloat16 [4096], P('ep'), may hold values from -0.09375 to 0.09375
- w_dense_gate: bfloat16 [4096, 1024], P('ep', 'tp'), may hold values from -0.09375 to 0.09375
- w_dense_up: bfloat16 [4096, 1024], P('ep', 'tp'), may hold values from -0.09375 to 0.09375
- w_dense_down: bfloat16 [1024, 4096], P('tp', 'ep'), may hold values from -0.1875 to 0.1875
- routes: int32 [1024, 4], replicated, may hold values from 0 to 63, all different within a row; in each aligned block of 16 rows (0 to 15, 16 to 31, ...) at most 2 rows name the same one
- route_weights: float32 [1024, 4], replicated, may hold values from 0.2 to 1.5
- w_exp_gate: bfloat16 [64, 4096, 1024], P('ep', None, 'tp'), may hold values from -0.09375 to 0.09375
- w_exp_up: bfloat16 [64, 4096, 1024], P('ep', None, 'tp'), may hold values from -0.09375 to 0.09375
- w_exp_down: bfloat16 [64, 1024, 4096], P('ep', 'tp'), may hold values from -0.1875 to 0.1875
Outputs:
- layer_out: bfloat16 [1024, 4096], P(None, 'ep')
- new_matrix: float32 [1024, 16, 64, 128], P('ep', 'tp')
- new_norm: float32 [1024, 16, 64], P('ep', 'tp')
- new_max: float32 [1024, 16], P('ep', 'tp')
The draws below stay inside these ranges and needn't reach their ends.
Inputs may be any that keep to these rules, and one draw needn't show every extreme that they name: `routes`: each row names 4 different experts. In the rows of one device (aligned blocks of 16 rows) no expert is named by more than 2 rows, a bound that some block reaches.
All inputs are finite; a program needn't handle non-finite values.
Results may differ from the reference program's by a relative error of at most 0.012.
Values may be sent and summed in bfloat16 or wider, within the bound.
No kernel may reach another device: no remote copies, remote signals or barrier semaphores. Data moves between devices by JAX's collectives and lax.ppermute only.
A program may use at most 128 MiB of HBM per device.

```python
import math
import jax
import jax.numpy as jnp
import numpy as np
from jax import lax

D = 4096
H = 16
DK = 64
DV = 128
FE = 1024
FS = 1024
TOPK = 4
SEQ_DEV = 16
HQK = 1024
HV = 2048
EXPERTS = 64
BATCH = 1024
CAP = 2
UNIT_GROUP = 256
N_EP = 64
N_TP = 4


def draw_tokens(key, part):
    base_key, scale_key, column_key = jax.random.split(key, 3)
    noise = jnp.clip(jax.random.normal(base_key, (BATCH, D), jnp.float32), -5.0, 5.0)
    row_scale = jnp.exp(jax.random.uniform(scale_key, (BATCH, 1), jnp.float32, math.log(0.4), math.log(2.5)))
    col_scale = 3.0 ** (jnp.arange(D, dtype=jnp.float32) / D) * jnp.exp(jax.random.uniform(column_key, (D,), jnp.float32, -0.35, 0.35))
    return (noise * row_scale * col_scale[None, :]).astype(jnp.bfloat16)


def level_of(rng, extent, cuts, least, top_value):
    loudness = 1.0
    for axis_at, blocks in cuts:
        steps = jax.random.uniform(jax.random.fold_in(jax.random.fold_in(rng, 6), axis_at), (blocks,), jnp.float32, least / len(cuts), top_value / len(cuts))
        loudness = loudness * jnp.repeat(jnp.exp(steps), extent[axis_at] // blocks).reshape((-1,) + (1,) * (len(extent) - 1 - axis_at))
    return loudness


def deal_out(rng, own, number, rows, amount, top, limit, lean):
    sequence = jax.random.permutation(rng, amount)
    heavy_load, common = load_shares(amount, rows * top, limit, lean, True), load_shares(amount, rows * top, limit, lean, False)
    places = jnp.arange(amount)

    def named(sizes, offset_by):
        used = int((sizes > 0).sum())
        fixed = max(1, used // 4)
        passed = fixed + (places - fixed + offset_by * (used - fixed)) % max(1, amount - fixed)
        return jnp.zeros((amount,), jnp.int32).at[sequence[jnp.where(places < fixed, places, passed)]].set(jnp.asarray(sizes, jnp.int32))

    sizes = jnp.where(number % 4 == 0, named(heavy_load, number // 4), named(common, number - number // 4 - 1))
    mixed = jax.random.permutation(jax.random.fold_in(own, 3), amount)
    source_of, receiver = mixed[0:amount // 2 * 2:2], mixed[1:amount // 2 * 2:2]
    room = jnp.minimum(sizes[source_of] - 1, limit - sizes[receiver]) // 2
    room = jnp.where((source_of == sequence[0]) | (receiver == sequence[0]) | (sizes[receiver] == 0), 0, jnp.maximum(room, 0))
    passed = jax.random.randint(jax.random.fold_in(own, 4), (amount // 2,), 0, 1 << 20) % (room + 1)
    sizes = sizes.at[source_of].add(-passed).at[receiver].add(passed)
    labels = jnp.searchsorted(jnp.cumsum(sizes), jnp.arange(rows * top), side="right").astype(jnp.int32)
    table = labels.reshape(top, rows).T
    table = table[jax.random.permutation(jax.random.fold_in(own, 1), rows)]
    offset_by = jax.random.randint(jax.random.fold_in(own, 2), (rows, 1), 0, top)
    return jnp.take_along_axis(table, (jnp.arange(top)[None, :] + offset_by) % top, axis=1)


def load_shares(count, total, bound, lean, full):
    weights = [(1 << 20) // math.isqrt(grade ** lean) + 1 for grade in range(1, count + 1)]
    largest = bound if full else min(bound, max(-(-total // count), total * weights[0] // sum(weights)))
    least = 1 if total - largest >= count - 1 else 0
    given, spare = [largest] + [least] * (count - 1), total - largest - least * (count - 1)
    while spare > 0:
        candidates = [i for i in range(1, count) if given[i] < largest] or [i for i in range(1, count) if given[i] < bound]
        whole, remaining = sum([weights[i] for i in candidates]), spare
        for i in candidates:
            extra = min(bound - given[i], max(1, remaining * weights[i] // whole), spare)
            given[i] = given[i] + extra
            spare = spare - extra
    return np.array(given)


def scatter_about(stream_key, shape, scale, reach, pieces=(), kind=jnp.bfloat16):
    array = scale * jax.random.normal(stream_key, shape, jnp.float32)
    if pieces:
        array = array * level_of(stream_key, shape, pieces, -0.22, 0.18)
    return jnp.clip(array, -reach, reach).astype(kind)


def setup_inputs(seed: int = 0) -> dict:
    keys = jax.random.split(jax.random.key(seed), 26)
    tokens = draw_tokens(jax.random.fold_in(keys[25], 71), 0)
    mix_gain = jnp.clip(1.0 + 0.18 * jax.random.normal(keys[1], (D,), jnp.float32), 0.099609375, 1.8984375).astype(jnp.bfloat16)
    w_query = scatter_about(keys[2], (D, HQK), D ** -0.5, 0.09375, ((0, 64), (1, 4)))
    w_key = scatter_about(keys[3], (D, HQK), D ** -0.5, 0.09375, ((0, 64), (1, 4)))
    w_value = scatter_about(keys[4], (D, HV), D ** -0.5, 0.09375, ((0, 64), (1, 4)))
    w_outgate = scatter_about(keys[5], (D, HV), D ** -0.5, 0.09375, ((0, 64), (1, 4)))
    w_igate = scatter_about(keys[6], (D, H), D ** -0.5, 0.09375, ((0, 64), (1, 4)))
    w_fgate = scatter_about(keys[7], (D, H), D ** -0.5, 0.09375, ((0, 64), (1, 4)))
    igate_bias = scatter_about(keys[8], (H,), 1.0, 3.0, ((0, 4),), jnp.float32)
    fgate_bias = jnp.clip(-1.0 + 4.0 * jax.random.uniform(keys[9], (H,), jnp.float32) ** level_of(keys[9], (H,), ((0, 4),), -0.2, 0.2), -1.0, 3.0)
    head_gain = jnp.clip(1.0 + 0.18 * jax.random.normal(keys[10], (HV,), jnp.float32), 0.099609375, 1.8984375).astype(jnp.bfloat16)
    w_mixout = scatter_about(keys[11], (HV, D), HV ** -0.5, 0.125, ((0, 4), (1, 64)))
    state_matrix = scatter_about(keys[12], (BATCH, H, DK, DV), 0.5, 3.0, ((0, 64), (1, 4)), jnp.float32)
    state_norm = scatter_about(keys[13], (BATCH, H, DK), 0.5, 3.0, ((0, 64), (1, 4)), jnp.float32)
    state_max = scatter_about(keys[14], (BATCH, H), 1.0, 3.0, ((0, 64), (1, 4)), jnp.float32)
    ffn_gain = jnp.clip(1.0 + 0.18 * jax.random.normal(keys[15], (D,), jnp.float32), 0.099609375, 1.8984375).astype(jnp.bfloat16)
    dense_mix = scatter_about(keys[16], (D,), D ** -0.5, 0.09375, ((0, 64),))
    w_dense_gate = scatter_about(keys[17], (D, FS), D ** -0.5, 0.09375, ((0, 64), (1, 4)))
    w_dense_up = scatter_about(keys[18], (D, FS), D ** -0.5, 0.09375, ((0, 64), (1, 4)))
    w_dense_down = scatter_about(keys[19], (FS, D), FS ** -0.5, 0.1875, ((0, 4), (1, 64)))
    routes_keys = jax.random.split(jax.random.fold_in(keys[20], 1), BATCH // SEQ_DEV)
    routes_turns = jax.random.permutation(jax.random.fold_in(keys[20], 3), BATCH // SEQ_DEV)
    routes = jax.vmap(lambda own, number: deal_out(jax.random.fold_in(keys[20], 2), own, number, SEQ_DEV, EXPERTS, TOPK, CAP, 2))(routes_keys, routes_turns).reshape((BATCH, TOPK))
    route_weights = jnp.clip(jnp.exp(jax.random.uniform(keys[21], (BATCH, TOPK), jnp.float32, math.log(0.2), math.log(1.5))), 0.2, 1.5)
    w_exp_gate = scatter_about(keys[22], (EXPERTS, D, FE), D ** -0.5, 0.09375, ((0, 64), (2, 4)))
    w_exp_up = scatter_about(keys[23], (EXPERTS, D, FE), D ** -0.5, 0.09375, ((0, 64), (2, 4)))
    w_exp_down = scatter_about(keys[24], (EXPERTS, FE, D), FE ** -0.5, 0.1875, ((0, 64), (1, 4)))
    return dict(tokens=tokens, mix_gain=mix_gain, w_query=w_query, w_key=w_key, w_value=w_value, w_outgate=w_outgate, w_igate=w_igate, w_fgate=w_fgate, igate_bias=igate_bias, fgate_bias=fgate_bias, head_gain=head_gain, w_mixout=w_mixout, state_matrix=state_matrix, state_norm=state_norm, state_max=state_max, ffn_gain=ffn_gain, dense_mix=dense_mix, w_dense_gate=w_dense_gate, w_dense_up=w_dense_up, w_dense_down=w_dense_down, routes=routes, route_weights=route_weights, w_exp_gate=w_exp_gate, w_exp_up=w_exp_up, w_exp_down=w_exp_down)


EPSILON = 1e-06
SOFT_CAP = 15.0

def gate_logs(in_pre, forget_pre, igate_bias, fgate_bias):
    in_log = SOFT_CAP * jnp.tanh((in_pre + igate_bias) / SOFT_CAP)
    forget_log = jax.nn.log_sigmoid(SOFT_CAP * jnp.tanh((forget_pre + fgate_bias) / SOFT_CAP))
    return (in_log, forget_log)

def recurrent_read(queries, keys_in, values_in, in_log, forget_log, state_matrix, state_norm, state_max):
    scaled_query = queries.astype(jnp.float32) * queries.shape[-1] ** (-0.5)
    key_float = keys_in.astype(jnp.float32)
    value_float = values_in.astype(jnp.float32)
    new_max = jnp.maximum(forget_log + state_max, in_log)
    carried = jnp.exp(forget_log + state_max - new_max)
    fresh_weight = jnp.exp(in_log - new_max)
    new_matrix = carried[..., None, None] * state_matrix + fresh_weight[..., None, None] * key_float[..., :, None] * value_float[..., None, :]
    new_norm = carried[..., None] * state_norm + fresh_weight[..., None] * key_float
    numerator = lax.optimization_barrier(jnp.sum(new_matrix * scaled_query[..., :, None], axis=-2))
    denominator = lax.optimization_barrier(jnp.sum(new_norm * scaled_query, axis=-1))
    floor_value = jnp.maximum(jnp.abs(denominator), jnp.exp(-new_max))
    readout = numerator / floor_value[..., None]
    return (readout, new_matrix, new_norm, new_max)

def head_output(readout, outgates, head_gain):
    scaled = readout * lax.rsqrt(lax.optimization_barrier(jnp.mean(readout * readout, axis=-1, keepdims=True)) + EPSILON)
    rows_count, heads_count, head_width = readout.shape
    gated_rows = scaled.reshape(rows_count, heads_count * head_width) * head_gain.astype(jnp.float32)[None, :]
    gated_rows = gated_rows * jax.nn.sigmoid(outgates.astype(jnp.float32))
    return gated_rows.astype(jnp.bfloat16)

def expert_slots(routes, groups, capacity, experts_all):
    row_total = routes.shape[0]
    chosen = (routes[:, :, None] == jnp.arange(experts_all, dtype=jnp.int32)[None, None, :]).astype(jnp.int32)
    per_row = lax.optimization_barrier(jnp.sum(chosen, axis=1))
    grouped = per_row.reshape(groups, row_total // groups, experts_all)
    earlier = (jnp.cumsum(grouped, axis=1) - grouped).reshape(row_total, experts_all)
    rank_in = lax.optimization_barrier(jnp.sum(chosen * earlier[:, None, :], axis=2))
    group_of = jnp.arange(row_total, dtype=jnp.int32) // (row_total // groups)
    return (routes * (groups * capacity) + group_of[:, None] * capacity + rank_in).astype(jnp.int32)

def reference(tokens, mix_gain, w_query, w_key, w_value, w_outgate, w_igate, w_fgate, igate_bias, fgate_bias, head_gain, w_mixout, state_matrix, state_norm, state_max, ffn_gain, dense_mix, w_dense_gate, w_dense_up, w_dense_down, routes, route_weights, w_exp_gate, w_exp_up, w_exp_down):
    token_float = tokens.astype(jnp.float32)
    inverse = lax.rsqrt(lax.optimization_barrier(jnp.mean(token_float * token_float, axis=1)) + EPSILON)
    normed = (token_float * inverse[:, None] * mix_gain.astype(jnp.float32)[None, :]).astype(jnp.bfloat16)
    queries = jnp.dot(normed, w_query, preferred_element_type=jnp.float32).astype(jnp.bfloat16).reshape(BATCH, H, DK)
    keys_in = jnp.dot(normed, w_key, preferred_element_type=jnp.float32).astype(jnp.bfloat16).reshape(BATCH, H, DK)
    values_in = jnp.dot(normed, w_value, preferred_element_type=jnp.float32).astype(jnp.bfloat16).reshape(BATCH, H, DV)
    outgates = jnp.dot(normed, w_outgate, preferred_element_type=jnp.float32).astype(jnp.bfloat16)
    in_pre = jnp.dot(normed, w_igate, preferred_element_type=jnp.float32)
    forget_pre = jnp.dot(normed, w_fgate, preferred_element_type=jnp.float32)
    in_log, forget_log = gate_logs(in_pre, forget_pre, igate_bias, fgate_bias)
    readout, new_matrix, new_norm, new_max = recurrent_read(queries, keys_in, values_in, in_log, forget_log, state_matrix, state_norm, state_max)
    heads_out = head_output(readout, outgates, head_gain)
    mixer = lax.optimization_barrier(jnp.dot(heads_out, w_mixout, preferred_element_type=jnp.float32).astype(jnp.bfloat16))
    hidden_state = lax.optimization_barrier((token_float + mixer.astype(jnp.float32)).astype(jnp.bfloat16))
    hidden_float = hidden_state.astype(jnp.float32)
    gain_float = ffn_gain.astype(jnp.float32)
    inverse_two = lax.rsqrt(lax.optimization_barrier(jnp.mean(hidden_float * hidden_float, axis=1)) + EPSILON)
    dense_gate = inverse_two * lax.optimization_barrier(jnp.sum(hidden_float * gain_float[None, :] * dense_mix.astype(jnp.float32)[None, :], axis=1))
    normed_two = (hidden_float * inverse_two[:, None] * gain_float[None, :]).astype(jnp.bfloat16)
    dense_hidden = (jax.nn.silu(jnp.dot(normed_two, w_dense_gate, preferred_element_type=jnp.float32)) * jnp.dot(normed_two, w_dense_up, preferred_element_type=jnp.float32)).astype(jnp.bfloat16)
    dense = jnp.dot(dense_hidden, w_dense_down, preferred_element_type=jnp.float32)
    flat_index = expert_slots(routes, N_EP, CAP, EXPERTS).reshape(-1)
    slot_count = N_EP * CAP
    send_rows = jnp.zeros((EXPERTS * slot_count, D), jnp.bfloat16).at[flat_index].set(jnp.repeat(normed_two, TOPK, axis=0)).reshape(EXPERTS, slot_count, D)

    def run_expert(operands):
        gate_matrix, up_matrix, down_matrix, arrived = operands
        gate_part = jnp.dot(arrived, gate_matrix, preferred_element_type=jnp.float32)
        up_part = jnp.dot(arrived, up_matrix, preferred_element_type=jnp.float32)
        expert_hidden = (jax.nn.silu(gate_part) * up_part).astype(jnp.bfloat16)
        summed = jnp.zeros((arrived.shape[0], D), jnp.float32)
        for group_index in range(N_TP):
            lower = group_index * UNIT_GROUP
            expert_part = jnp.dot(expert_hidden[:, lower:lower + UNIT_GROUP], down_matrix[lower:lower + UNIT_GROUP], preferred_element_type=jnp.float32).astype(jnp.bfloat16)
            summed = summed + lax.optimization_barrier(expert_part).astype(jnp.float32)
        return summed
    returned = lax.map(run_expert, (w_exp_gate, w_exp_up, w_exp_down, send_rows))
    picked = returned.reshape(EXPERTS * slot_count, D)[flat_index].reshape(BATCH, TOPK, D)
    routed = lax.optimization_barrier(jnp.sum(picked * route_weights[:, :, None], axis=1))
    layer_out = (hidden_float + routed + jax.nn.sigmoid(dense_gate)[:, None] * dense).astype(jnp.bfloat16)
    return (layer_out, new_matrix, new_norm, new_max)
```

```python
import functools

import jax
import jax.numpy as jnp
from jax import lax
from jax.experimental import pallas as pl
from jax.experimental.pallas import tpu as pltpu
from jax.sharding import Mesh
from jax.sharding import PartitionSpec as P


D = 4096


EPSILON = 1e-06
SOFT_CAP = 15.0
NZ, NY, NC, NX = 8, 4, 2, 4
EP = ("z", "y", "c")
F32, BF16 = jnp.float32, jnp.bfloat16


def exchanged(x, axis):
    return lax.all_to_all(x, axis, split_axis=0, concat_axis=0, tiled=True)


def to_all(x, axis):
    return exchanged(jnp.broadcast_to(x, (lax.axis_size(axis), *x.shape)), axis)


def other_core(x):
    return lax.ppermute(x, "c", [(0, 1), (1, 0)])


def stacked_kernel(*refs):
    for i in range(NZ):
        refs[-1][i] = refs[i][...]


def gathered_z(x):
    pieces = [x] + [
        lax.ppermute(x, "z", [(i, (i + s) % NZ) for i in range(NZ)]) for s in range(1, NZ)
    ]
    zs = pl.pallas_call(
        stacked_kernel,
        out_shape=jax.ShapeDtypeStruct((NZ, *x.shape), x.dtype),
        in_specs=[VMEM] * NZ,
        out_specs=VMEM,
        cost_estimate=pl.CostEstimate(flops=1 << 20, bytes_accessed=2 << 20, transcendentals=0),
        name="stacked",
    )(*pieces)
    return zs, other_core(zs)


def over_x(x):
    return to_all(x, "x").astype(F32).sum(axis=0)


def packed(x):
    h = x.shape[0] // 2
    return jnp.concatenate([x[:h], x[h:]], axis=1)


def unpacked(x):
    return jnp.concatenate([x[:, :64], x[:, 64:]], axis=0)


def turned_z(place_ref, z):
    az = lax.rem(place_ref[2] + (NZ - z), NZ)
    return pl.ds(pl.multiple_of(az * 128, 128), 128)


def mix_kernel(c_ref, h_ref, mine_ref, away_ref, out_ref):
    c = c_ref[0]
    both = jnp.concatenate(
        [h_ref[y, :16, :256] for y in range(NY)] + [h_ref[y, :16, 256:] for y in range(NY)], axis=0
    )
    lane = lax.broadcasted_iota(jnp.int32, (64, 128), 1)
    for z in range(NZ):
        res = []
        for w in (mine_ref, away_ref):
            r = jnp.dot(both, w[z, :256, :], preferred_element_type=F32)
            top, low = r[:64], r[64:]
            res.append((top + pltpu.roll(low, 64, 1), pltpu.roll(top, 64, 1) + low))
        first = jnp.where(c == 0, res[0][0], res[1][0])
        second = jnp.where(c == 0, res[1][1], res[0][1])
        tile = jnp.where(lane < 64, first, second).astype(BF16)
        for y in range(NY):
            out_ref[y, :, turned_z(c_ref, z)] = tile[y * 16 : (y + 1) * 16]


VMEM = pl.BlockSpec(memory_space=pltpu.VMEM)
SMEM = pl.BlockSpec(memory_space=pltpu.SMEM)


def mix(c, heads, mine, away):
    return pl.pallas_call(
        mix_kernel,
        out_shape=jax.ShapeDtypeStruct((NY, 16, 1024), BF16),
        in_specs=[SMEM, VMEM, VMEM, VMEM],
        out_specs=VMEM,
        cost_estimate=pl.CostEstimate(
            flops=2 * 128 * 256 * 128 * 16, bytes_accessed=2 << 20, transcendentals=0
        ),
        name="mix",
    )(c, heads, mine, away)


def settle_kernel(
    c_ref, got_ref, tok_ref, gain_ref, mix_ref, spread_ref,
    hid_ref, gate_ref, send_ref, n0_ref, n1_ref, n2_ref, n3_ref, norm_ref,
):
    square = jnp.zeros((16, 1), F32)
    dot = jnp.zeros((16, 1), F32)
    for y in range(NY):
        total = got_ref[y, 0].astype(F32)
        for x in range(1, NX):
            total += got_ref[y, x].astype(F32)
        total = total.astype(BF16).astype(F32)
        for z in range(NZ):
            at = (z * NY + y) * 128
            cols = slice(at, at + 128)
            hid = (tok_ref[:, cols].astype(F32) + total[:, z * 128 : (z + 1) * 128]).astype(BF16)
            hid_ref[:, cols] = hid
            wide = hid.astype(F32)
            square += jnp.sum(wide * wide, axis=1, keepdims=True)
            dot += jnp.sum(wide * gain_ref[:, cols] * mix_ref[:, cols], axis=1, keepdims=True)
    inverse = lax.rsqrt(square / D + EPSILON)
    gate_ref[...] = jnp.broadcast_to(1.0 / (1.0 + jnp.exp(-(inverse * dot))), (16, 128))
    spread = spread_ref[...]
    for at in range(0, D, 512):
        cols = slice(at, at + 512)
        norm = (hid_ref[:, cols].astype(F32) * inverse * gain_ref[:, cols]).astype(BF16)
        norm_ref[:, cols] = norm
        send_ref[:, cols] = jnp.dot(spread, norm, preferred_element_type=F32).astype(BF16)
    for s, out in enumerate((n0_ref, n1_ref, n2_ref, n3_ref)):
        to = lax.rem(c_ref[1] + s, NY)
        for z in range(NZ):
            at = pl.multiple_of((z * NY + to) * 128, 128)
            out[:, z * 128 : (z + 1) * 128] = norm_ref[:, pl.ds(at, 128)]


def settle(c, got, tok, gain, mix_row, spread):
    part = jax.ShapeDtypeStruct((16, 1024), BF16)
    return pl.pallas_call(
        settle_kernel,
        out_shape=(
            jax.ShapeDtypeStruct((16, D), BF16),
            jax.ShapeDtypeStruct((16, 128), F32),
            jax.ShapeDtypeStruct((128, D), BF16),
            part, part, part, part,
        ),
        in_specs=[SMEM] + [VMEM] * 5,
        out_specs=(VMEM,) * 7,
        scratch_shapes=[pltpu.VMEM((16, D), BF16)],
        cost_estimate=pl.CostEstimate(
            flops=2 * 128 * 128 * 4096, bytes_accessed=3 << 20, transcendentals=0
        ),
        name="settle",
    )(c, got, tok, gain, mix_row, spread)


def dense_kernel(c_ref, x0, x1, x2, x3, mine_ref, away_ref, o0, o1, o2, o3):
    c = c_ref[0]
    acc = [jnp.zeros((64, 128), F32) for _ in range(4)]
    for z in range(NZ):
        cols = turned_z(c_ref, z)
        x = jnp.concatenate([r[:, cols] for r in (x0, x1, x2, x3)], axis=0)
        own = jnp.where(c == 0, x[:, :64], x[:, 64:])
        off = jnp.where(c == 0, x[:, 64:], x[:, :64])
        for j in range(4):
            rows = slice(272 + j * 64, 336 + j * 64)
            acc[j] += jnp.dot(own, mine_ref[z, rows, :], preferred_element_type=F32)
            acc[j] += jnp.dot(off, away_ref[z, rows, :], preferred_element_type=F32)
    for s, out in enumerate((o0, o1, o2, o3)):
        for j in range(4):
            out[:, j * 128 : (j + 1) * 128] = acc[j][s * 16 : (s + 1) * 16].astype(BF16)


def dense_products(c, xs, mine, away):
    part = jax.ShapeDtypeStruct((16, 512), BF16)
    return pl.pallas_call(
        dense_kernel,
        out_shape=(part,) * 4,
        in_specs=[SMEM] + [VMEM] * 6,
        out_specs=(VMEM,) * 4,
        cost_estimate=pl.CostEstimate(
            flops=2 * 64 * 1024 * 512, bytes_accessed=2 << 20, transcendentals=0
        ),
        name="dense_products",
    )(c, *xs, mine, away)


def dense_down_kernel(c_ref, x0, x1, x2, x3, mine_ref, away_ref, o0, o1, o2, o3):
    c = c_ref[0]
    xs = (x0, x1, x2, x3)
    both = jnp.concatenate([r[:, :128] for r in xs] + [r[:, 128:] for r in xs], axis=0)
    lane = lax.broadcasted_iota(jnp.int32, (64, 128), 1)
    for z in range(NZ):
        res = []
        for w in (mine_ref, away_ref):
            r = jnp.dot(both, w[z, 528:656, :], preferred_element_type=F32)
            top, low = r[:64], r[64:]
            res.append((top + pltpu.roll(low, 64, 1), pltpu.roll(top, 64, 1) + low))
        first = jnp.where(c == 0, res[0][0], res[1][0])
        second = jnp.where(c == 0, res[1][1], res[0][1])
        tile = jnp.where(lane < 64, first, second).astype(BF16)
        for s, out in enumerate((o0, o1, o2, o3)):
            out[:, turned_z(c_ref, z)] = tile[s * 16 : (s + 1) * 16]


def dense_down(c, xs, mine, away):
    part = jax.ShapeDtypeStruct((16, 1024), BF16)
    return pl.pallas_call(
        dense_down_kernel,
        out_shape=(part,) * 4,
        in_specs=[SMEM] + [VMEM] * 6,
        out_specs=(VMEM,) * 4,
        cost_estimate=pl.CostEstimate(
            flops=2 * 64 * 1024 * 512, bytes_accessed=1 << 20, transcendentals=0
        ),
        name="dense_down",
    )(c, *xs, mine, away)


def half_rows(tile):
    lane = lax.broadcasted_iota(jnp.int32, (8, 128), 1)
    wide = tile.astype(F32)
    turn = pltpu.roll(wide, 64, 1)
    return (
        jnp.where(lane < 64, wide[:8], turn[8:]),
        jnp.where(lane < 64, turn[:8], wide[8:]),
    )


def down_kernel(c_ref, h_ref, w_ref, hid_ref, d0, d1, d2, d3, out_ref):
    res = jnp.dot(h_ref[...], w_ref[...], preferred_element_type=F32)
    lane = lax.broadcasted_iota(jnp.int32, (64, 128), 1)
    for p in range(8):
        cols = slice(p * 128, (p + 1) * 128)
        top, low = res[:64, cols], res[64:, cols]
        out_ref[2 * p, :64] = jnp.where(lane < 64, top, pltpu.roll(low, 64, 1)).astype(BF16)
        out_ref[2 * p + 1, :64] = jnp.where(lane < 64, pltpu.roll(top, 64, 1), low).astype(BF16)
    for zl in range(2):
        for s, d in enumerate((d0, d1, d2, d3)):
            at = zl * NY + lax.rem(c_ref[1] + s, NY)
            hid = half_rows(hid_ref[:, pl.ds(pl.multiple_of(at * 128, 128), 128)])
            den = half_rows(d[:, zl * 128 : (zl + 1) * 128])
            for k in range(2):
                out_ref[2 * at + k, 64:] = jnp.concatenate([hid[k], den[k]], axis=0).astype(BF16)


def down_for_all(c, expert_hidden, w, hidden, downs):
    return pl.pallas_call(
        down_kernel,
        grid=(4,),
        out_shape=jax.ShapeDtypeStruct((64, 80, 128), BF16),
        in_specs=[
            SMEM,
            pl.BlockSpec((128, 256), lambda i: (0, 0)),
            pl.BlockSpec((256, 1024), lambda i: (0, i)),
            pl.BlockSpec((16, 1024), lambda i: (0, i)),
        ]
        + [pl.BlockSpec((16, 256), lambda i: (0, i))] * 4,
        out_specs=pl.BlockSpec((16, 80, 128), lambda i: (i, 0, 0)),
        cost_estimate=pl.CostEstimate(
            flops=2 * 128 * 256 * 4096, bytes_accessed=4 << 20, transcendentals=0
        ),
        name="down",
    )(c, expert_hidden, w, hidden, *downs)


def project_kernel(kept, c_ref, tok_ref, gain_ref, q_ref, k_ref, v_ref, o_ref, i_ref, f_ref, out, all_ref, x_ref):
    core = c_ref[0] if kept else 1 - c_ref[0]
    gain = gain_ref[...].astype(F32)
    lane = lax.broadcasted_iota(jnp.int32, (128, 128), 1)
    all_ref[...] = jnp.transpose(tok_ref[...])
    gate_rows = jnp.concatenate(
        [jnp.zeros((64, 64), BF16), i_ref[...], f_ref[...], jnp.zeros((56, 64), BF16)], axis=0
    )
    for y in range(NY):
        for z in range(NZ):
            at = pl.multiple_of(((z * NY + y) * NC + core) * 16, 16)
            x_ref[z * 16 : (z + 1) * 16, :] = all_ref[pl.ds(at, 16), :]
        wide = x_ref[...].astype(F32)
        scaled = (wide * gain).astype(BF16)
        rows = slice(y * 128, (y + 1) * 128)
        at = 0
        for w in (q_ref, k_ref, v_ref, o_ref):
            n = w.shape[1]
            res = jnp.dot(scaled, w[...], preferred_element_type=F32)
            out[rows, at : at + n] = res.astype(out.dtype)
            at += n
        gates = lax.dot_general(
            scaled, gate_rows, (((1,), (1,)), ((), ())), preferred_element_type=F32
        )
        square = jnp.sum(wide * wide, axis=1, keepdims=True)
        both = jnp.concatenate([wide, jnp.zeros((128, 64), F32)], axis=1)
        last = jnp.where(lane < 64, both, jnp.where(lane == 72, square, gates))
        out[rows, 1536:1664] = last.astype(out.dtype)


def project(kept, *args):
    return pl.pallas_call(
        functools.partial(project_kernel, kept),
        out_shape=jax.ShapeDtypeStruct((512, 1664), F32 if kept else BF16),
        in_specs=[SMEM] + [VMEM] * 8,
        out_specs=VMEM,
        scratch_shapes=[pltpu.VMEM((1024, 64), BF16), pltpu.VMEM((128, 64), BF16)],
        cost_estimate=pl.CostEstimate(
            flops=2 * 512 * 256 * 1664, bytes_accessed=3 << 20, transcendentals=0
        ),
        name="project_kept" if kept else "project_away",
    )(*args)


def fold_core_kernel(c_ref, kept_ref, got_ref, out_ref):
    c = c_ref[0]
    lane = lax.broadcasted_iota(jnp.int32, (128, 128), 1)
    for y in range(NY):
        rows = slice(y * 128, (y + 1) * 128)
        kept, got = kept_ref[rows, :], got_ref[rows, :].astype(F32)
        out_ref[y, :, :1664] = (kept + got).astype(BF16)
        a, b = kept[:, 1536:], got[:, 1536:]
        first = jnp.where(c == 0, a, b)
        second = jnp.where(c == 0, b, a)
        out_ref[y, :, 1664:] = jnp.where(lane < 64, first, pltpu.roll(second, 64, 1)).astype(BF16)


def fold_core(c, kept, got):
    return pl.pallas_call(
        fold_core_kernel,
        out_shape=jax.ShapeDtypeStruct((NY, 128, 1792), BF16),
        in_specs=[SMEM, VMEM, VMEM],
        out_specs=VMEM,
        cost_estimate=pl.CostEstimate(
            flops=1 << 20, bytes_accessed=6 << 20, transcendentals=0
        ),
        name="fold_core",
    )(c, kept, got)


def fold_y_kernel(in_ref, out_ref):
    for z in range(NZ):
        rows = slice(z * 16, (z + 1) * 16)
        total = in_ref[0, rows, :1664].astype(F32)
        for y in range(1, NY):
            total += in_ref[y, rows, :1664].astype(F32)
        out_ref[z, :, :1664] = total.astype(BF16)
        for y in range(NY):
            at = 1664 + y * 128
            out_ref[z, :, at : at + 128] = in_ref[y, rows, 1664:]


def fold_y(x):
    return pl.pallas_call(
        fold_y_kernel,
        out_shape=jax.ShapeDtypeStruct((NZ, 16, 2176), BF16),
        in_specs=[VMEM],
        out_specs=VMEM,
        cost_estimate=pl.CostEstimate(
            flops=1 << 20, bytes_accessed=3 << 20, transcendentals=0
        ),
        name="fold_y",
    )(x)


def recur_kernel(
    in_ref, ib_ref, fb_ref, hg_ref, sm_ref, sn_ref, mx_ref,
    heads_ref, tok_ref, nm_ref, nn_ref, nx_ref,
    kt_ref, qt_ref, car_ref, flo_ref, val_ref, out_ref, num_ref,
):
    g = pl.program_id(0)

    @pl.when(g == 0)
    def _():
        total = in_ref[0, :, :1664].astype(F32)
        for z in range(1, NZ):
            total += in_ref[z, :, :1664].astype(F32)
        for z in range(NZ):
            for y in range(NY):
                at, src = (z * NY + y) * 128, 1664 + y * 128
                tok_ref[:, at : at + 128] = in_ref[z, :, src : src + 128]
        inverse = lax.rsqrt(total[:, 1608:1609] / D + EPSILON)
        total = total * inverse
        q = total[:, :256].astype(BF16).astype(F32) * 0.125
        k = total[:, 256:512].astype(BF16).astype(F32)
        for h in range(4):
            cols = slice(512 + h * 128, 640 + h * 128)
            val_ref[h] = total[:, cols].astype(BF16).astype(F32)
        out_ref[...] = total[:, 1024:1536].astype(BF16).astype(F32)
        in_log = SOFT_CAP * jnp.tanh((total[:, 1600:1604] + ib_ref[...]) / SOFT_CAP)
        f = SOFT_CAP * jnp.tanh((total[:, 1604:1608] + fb_ref[...]) / SOFT_CAP)
        forget_log = jnp.minimum(f, 0.0) - jnp.log1p(jnp.exp(-jnp.abs(f)))
        kept = forget_log + mx_ref[...]
        top = jnp.maximum(kept, in_log)
        nx_ref[...] = top
        carried = jnp.exp(kept - top)
        fresh = jnp.exp(in_log - top)
        least = jnp.exp(-top)
        scaled = []
        for h in range(4):
            cols = slice(h * 64, (h + 1) * 64)
            fk = fresh[:, h : h + 1] * k[:, cols]
            scaled.append(fk)
            norm = carried[:, h : h + 1] * sn_ref[:, h, :] + fk
            nn_ref[:, h, :] = norm
            den = jnp.abs(jnp.sum(norm * q[:, cols], axis=1, keepdims=True))
            flo_ref[h] = jnp.broadcast_to(jnp.maximum(den, least[:, h : h + 1]), (16, 128))
            car_ref[h] = jnp.broadcast_to(carried[:, h : h + 1], (16, 128))
        kt = jnp.transpose(jnp.concatenate(scaled, axis=1))
        qt = jnp.transpose(q)
        for i in range(4):
            kt_ref[i] = kt[:, i * 4 : (i + 1) * 4]
            qt_ref[i] = qt[:, i * 4 : (i + 1) * 4]

    for i in range(4):
        b = g * 4 + i
        for h in range(4):
            rows = slice(h * 64, (h + 1) * 64)
            new = (
                car_ref[h, pl.ds(b, 1), :] * sm_ref[i, h]
                + kt_ref[g, rows, i : i + 1] * val_ref[h, pl.ds(b, 1), :]
            )
            nm_ref[i, h] = new
            num_ref[h, pl.ds(b, 1), :] = jnp.sum(
                new * qt_ref[g, rows, i : i + 1], axis=0, keepdims=True
            )

    @pl.when(g == 3)
    def _():
        for h in range(4):
            cols = slice(h * 128, (h + 1) * 128)
            read = num_ref[h] / flo_ref[h]
            mean = jnp.mean(read * read, axis=1, keepdims=True)
            gate = 1.0 / (1.0 + jnp.exp(-out_ref[:, cols]))
            scaled = read * lax.rsqrt(mean + EPSILON) * hg_ref[:, cols].astype(F32)
            heads_ref[:, cols] = (scaled * gate).astype(BF16)


def recur(x, igate_bias, fgate_bias, head_gain, state_matrix, state_norm, state_max):
    whole = lambda *shape: pl.BlockSpec(shape, lambda g: (0,) * len(shape))
    block = pl.BlockSpec((4, 4, 64, 128), lambda g: (g, 0, 0, 0))
    return pl.pallas_call(
        recur_kernel,
        grid=(4,),
        out_shape=(
            jax.ShapeDtypeStruct((16, 512), BF16),
            jax.ShapeDtypeStruct((16, D), BF16),
            jax.ShapeDtypeStruct((16, 4, 64, 128), F32),
            jax.ShapeDtypeStruct((16, 4, 64), F32),
            jax.ShapeDtypeStruct((16, 4), F32),
        ),
        in_specs=[
            whole(NZ, 16, 2176), whole(1, 4), whole(1, 4), whole(1, 512),
            block, whole(16, 4, 64), whole(16, 4),
        ],
        out_specs=(whole(16, 512), whole(16, D), block, whole(16, 4, 64), whole(16, 4)),
        scratch_shapes=[
            pltpu.VMEM((4, 256, 4), F32),
            pltpu.VMEM((4, 256, 4), F32),
            pltpu.VMEM((4, 16, 128), F32),
            pltpu.VMEM((4, 16, 128), F32),
            pltpu.VMEM((4, 16, 128), F32),
            pltpu.VMEM((16, 512), F32),
            pltpu.VMEM((4, 16, 128), F32),
        ],
        cost_estimate=pl.CostEstimate(
            flops=8 << 20, bytes_accessed=5 << 20, transcendentals=1 << 14
        ),
        name="recur",
    )(x, igate_bias[None], fgate_bias[None], head_gain[None], state_matrix, state_norm, state_max)


def slot_ranks(routes):
    chosen = (routes[:, :, None] == jnp.arange(64, dtype=jnp.int32)[None, None, :]).astype(F32)
    per_row = jnp.sum(chosen, axis=1).reshape(64, 16, 64)
    lower = jnp.tril(jnp.ones((16, 16), F32), -1)
    earlier = jnp.einsum("rs,gse->gre", lower, per_row).reshape(1024, 64)
    return jnp.sum(chosen * earlier[:, None, :], axis=2).astype(jnp.int32)


def layer(
    tokens,
    mix_gain,
    w_query,
    w_key,
    w_value,
    w_outgate,
    w_igate,
    w_fgate,
    igate_bias,
    fgate_bias,
    head_gain,
    w_mixout,
    state_matrix,
    state_norm,
    state_max,
    ffn_gain,
    dense_mix,
    w_dense_gate,
    w_dense_up,
    w_dense_down,
    routes,
    route_weights,
    w_exp_gate,
    w_exp_up,
    w_exp_down,
):
    me = lax.axis_index(EP)
    c = lax.axis_index("c")
    y, z = lax.axis_index("y"), lax.axis_index("z")
    c_ref = jnp.stack([c, y, z]).astype(jnp.int32)
    piece = jnp.concatenate(
        [
            packed(w_mixout),
            jnp.stack([jnp.pad(ffn_gain, (0, 64)), jnp.pad(dense_mix, (0, 64))]),
            jnp.zeros((14, 128), BF16),
            w_dense_gate[:, :128],
            w_dense_gate[:, 128:],
            w_dense_up[:, :128],
            w_dense_up[:, 128:],
            packed(w_dense_down),
        ],
        axis=0,
    )
    operands = (
        c_ref, tokens.T, mix_gain[None], w_query, w_key, w_value, w_outgate, w_igate.T, w_fgate.T
    )
    away = project(False, *operands)
    got = other_core(away)
    kept = project(True, *operands)
    folded = fold_core(c_ref, kept, got)
    folded = exchanged(folded, "y")
    folded = fold_y(folded)
    folded = exchanged(folded, "z")
    heads_out, tok, new_matrix, new_norm, new_max = recur(
        folded, igate_bias, fgate_bias, head_gain, state_matrix, state_norm, state_max
    )
    mine, away = gathered_z(piece)
    extra = jnp.stack([mine[:, 256:258, :64], away[:, 256:258, :64]])
    extra = jnp.where(c == 0, extra, extra[::-1])[:, (z - jnp.arange(NZ)) % NZ]
    extra = extra.transpose(2, 1, 0, 3).reshape(4, 512)
    heads = jnp.concatenate([heads_out, extra, jnp.zeros((4, 512), BF16)], axis=0)
    heads = to_all(heads, "y")
    vectors = heads[:, 16:20].reshape(NY, 2, NZ, 128).transpose(1, 2, 0, 3).reshape(2, 1, D)
    vectors = vectors.astype(F32)
    partial = mix(c_ref, heads, mine, away)
    copies = jnp.broadcast_to(partial[:, None], (NY, NX, 16, 1024)).reshape(16, 16, 1024)
    got = exchanged(copies, ("y", "x")).reshape(NY, NX, 16, 1024)
    ranks = slot_ranks(routes)
    target = routes * 2 + ranks
    own_target = lax.dynamic_slice(target, (me * 16, 0), (16, 4))
    slots = jnp.arange(128)
    spread = jnp.any(own_target[:, :, None] == slots[None, None, :], axis=1).T.astype(BF16)
    hidden, dense_gate, send, *sides = settle(c_ref, got, tok, vectors[0], vectors[1], spread)
    arrived = exchanged(send.reshape(64, 2, D), EP).reshape(128, D)
    xs = [sides[0]] + [
        lax.ppermute(sides[s], "y", [(i, (i + s) % NY) for i in range(NY)]) for s in (1, 2, 3)
    ]
    sums = dense_products(c_ref, xs, mine, away)
    parts = [sums[0]] + [
        lax.ppermute(sums[s], "y", [(i, (i - s) % NY) for i in range(NY)]) for s in (1, 2, 3)
    ]
    dense_sum = sum(p.astype(F32) for p in parts)
    dense_hidden = (
        jax.nn.silu(dense_sum[:, :256]) * dense_sum[:, 256:] * dense_gate[:, :1]
    ).astype(BF16)
    units = [dense_hidden] + [
        lax.ppermute(dense_hidden, "y", [(i, (i + s) % NY) for i in range(NY)])
        for s in (1, 2, 3)
    ]
    downs = dense_down(c_ref, units, mine, away)
    downs = [downs[0]] + [
        lax.ppermute(downs[s], "y", [(i, (i - s) % NY) for i in range(NY)]) for s in (1, 2, 3)
    ]
    named = routes == me
    slot_of = jnp.sum(jnp.where(named, (jnp.arange(1024) // 16)[:, None] * 2 + ranks, 0), axis=1)
    slot_weight = jnp.sum(jnp.where(named, route_weights, 0.0), axis=1)
    slot_hit = (slot_of[:, None] == slots[None, :]) & jnp.any(named, axis=1)[:, None]
    weight = jnp.sum(jnp.where(slot_hit, slot_weight[:, None], 0.0), axis=0)
    gate_part = jnp.dot(arrived, w_exp_gate[0], preferred_element_type=F32)
    up_part = jnp.dot(arrived, w_exp_up[0], preferred_element_type=F32)
    expert_hidden = (jax.nn.silu(gate_part) * up_part * weight[:, None]).astype(BF16)
    returned = down_for_all(c_ref, expert_hidden, w_exp_down[0], hidden, downs)
    returned = exchanged(returned, EP)
    rows = returned[:, 64:].reshape(64, 2, 8, 2, 64).transpose(1, 0, 3, 2, 4).reshape(2, 1024, 64)
    hidden_cols, dense_rows = rows[0], rows[1]
    returned = returned[:, :64]
    local = routes * 16 + 2 * ((jnp.arange(1024) // 16)[:, None] % 8) + ranks
    pick = jnp.any(local[:, :, None] == jnp.arange(1024)[None, None, :], axis=1).astype(BF16)
    pick = pick.reshape(2, 4, 128, 1024)
    source = returned.reshape(64, 4, 16, 128).transpose(1, 0, 2, 3).reshape(4, 1024, 128)
    halves = jnp.einsum("hgmk,gkn->hgmn", pick, source, preferred_element_type=F32)
    routed = jnp.concatenate(
        [halves[0, :, :, :64].reshape(512, 64), halves[1, :, :, 64:].reshape(512, 64)], axis=0
    )
    branch = packed((routed + dense_rows.astype(F32)).astype(BF16))
    branch = unpacked(over_x(branch))
    layer_out = (hidden_cols.astype(F32) + branch).astype(BF16)
    return (layer_out, new_matrix, new_norm, new_max)


def solution(mesh):
    return jax.shard_map(
        layer,
        mesh=Mesh(mesh.devices.reshape(NZ, NY, NC, NX), ("z", "y", "c", "x")),
        in_specs=(
            P(None, EP),
            P(EP),
            P(EP, "x"),
            P(EP, "x"),
            P(EP, "x"),
            P(EP, "x"),
            P(EP, "x"),
            P(EP, "x"),
            P("x"),
            P("x"),
            P("x"),
            P("x", EP),
            P(EP, "x", None, None),
            P(EP, "x", None),
            P(EP, "x"),
            P(EP),
            P(EP),
            P(EP, "x"),
            P(EP, "x"),
            P("x", EP),
            P(),
            P(),
            P(EP, None, "x"),
            P(EP, None, "x"),
            P(EP, "x", None),
        ),
        out_specs=(P(None, EP), P(EP, "x", None, None), P(EP, "x", None), P(EP, "x")),
        check_vma=False,
    )
```

```python
import functools

import jax
import jax.numpy as jnp
from jax import lax
from jax.experimental import pallas as pl
from jax.experimental.pallas import tpu as pltpu
from jax.sharding import Mesh
from jax.sharding import PartitionSpec as P


D = 4096


EPSILON = 1e-06
SOFT_CAP = 15.0
NZ, NY, NC, NX = 8, 4, 2, 4
EP = ("z", "y", "c")
F32, BF16 = jnp.float32, jnp.bfloat16
LIMIT = 16 << 20


def exchanged(x, axis):
    return lax.all_to_all(x, axis, split_axis=0, concat_axis=0, tiled=True)


def other_core(x):
    return lax.ppermute(x, "c", [(0, 1), (1, 0)])


def stacked_kernel(*refs):
    for i in range(NZ):
        refs[-1][i] = refs[i][...]


def gathered_z(x):
    pieces = [x] + [None] * (NZ - 1)
    up, down = x, x
    for s in range(1, NZ // 2 + 1):
        up = lax.ppermute(up, "z", [(i, (i + 1) % NZ) for i in range(NZ)])
        pieces[s] = up
        if s < NZ // 2:
            down = lax.ppermute(down, "z", [(i, (i - 1) % NZ) for i in range(NZ)])
            pieces[NZ - s] = down
    zs = pl.pallas_call(
        stacked_kernel,
        out_shape=jax.ShapeDtypeStruct((NZ, *x.shape), x.dtype),
        in_specs=[VMEM] * NZ,
        out_specs=VMEM,
        cost_estimate=pl.CostEstimate(flops=1 << 20, bytes_accessed=2 << 20, transcendentals=0),
        name="stacked",
    )(*pieces)
    return zs, other_core(zs)


def packed(x):
    h = x.shape[0] // 2
    return jnp.concatenate([x[:h], x[h:]], axis=1)


def turned_z(place_ref, z):
    az = lax.rem(place_ref[2] + (NZ - z), NZ)
    return pl.ds(pl.multiple_of(az * 128, 128), 128)


def both_kinds(c, r, n):
    lane = lax.broadcasted_iota(jnp.int32, (n, 128), 1)
    res = []
    for k in range(2):
        top, low = r[:n, k * 128 : (k + 1) * 128], r[n:, k * 128 : (k + 1) * 128]
        res.append((top + pltpu.roll(low, 64, 1), pltpu.roll(top, 64, 1) + low))
    first = jnp.where(c == 0, res[0][0], res[1][0])
    second = jnp.where(c == 0, res[1][1], res[0][1])
    return jnp.where(lane < 64, first, second).astype(BF16)


def mix_kernel(c_ref, x0, x1, x2, x3, mine_ref, away_ref, out_ref):
    c = c_ref[0]
    xs = (x0, x1, x2, x3)
    both = jnp.concatenate([r[:16, :256] for r in xs] + [r[:16, 256:] for r in xs], axis=0)
    for z in range(NZ):
        w = jnp.concatenate([mine_ref[z, :256, :], away_ref[z, :256, :]], axis=1)
        tile = both_kinds(c, jnp.dot(both, w, preferred_element_type=F32), 64)
        for s in range(NY):
            to = lax.rem(c_ref[1] + (NY - s), NY)
            out_ref[to, :, turned_z(c_ref, z)] = tile[s * 16 : (s + 1) * 16]


VMEM = pl.BlockSpec(memory_space=pltpu.VMEM)
SMEM = pl.BlockSpec(memory_space=pltpu.SMEM)


def mix(c, heads, mine, away):
    return pl.pallas_call(
        mix_kernel,
        out_shape=jax.ShapeDtypeStruct((NY, 16, 1024), BF16),
        in_specs=[SMEM] + [VMEM] * 6,
        out_specs=VMEM,
        compiler_params=pltpu.CompilerParams(vmem_limit_bytes=LIMIT),
        cost_estimate=pl.CostEstimate(
            flops=2 * 128 * 256 * 128 * 16, bytes_accessed=2 << 20, transcendentals=0
        ),
        name="mix",
    )(c, *heads, mine, away)


def settle_kernel(
    c_ref, got_ref, tok_ref, gain_ref, mix_ref, spread_ref,
    hid_ref, gate_ref, send_ref, n0_ref, n1_ref, n2_ref, n3_ref, norm_ref,
):
    square = jnp.zeros((16, 1), F32)
    dot = jnp.zeros((16, 1), F32)
    for y in range(NY):
        total = got_ref[y, 0].astype(F32)
        for x in range(1, NX):
            total += got_ref[y, x].astype(F32)
        total = total.astype(BF16).astype(F32)
        for z in range(NZ):
            at = (z * NY + y) * 128
            cols = slice(at, at + 128)
            hid = (tok_ref[:, cols].astype(F32) + total[:, z * 128 : (z + 1) * 128]).astype(BF16)
            hid_ref[:, cols] = hid
            wide = hid.astype(F32)
            square += jnp.sum(wide * wide, axis=1, keepdims=True)
            dot += jnp.sum(wide * gain_ref[:, cols] * mix_ref[:, cols], axis=1, keepdims=True)
    inverse = lax.rsqrt(square / D + EPSILON)
    gate_ref[...] = jnp.broadcast_to(1.0 / (1.0 + jnp.exp(-(inverse * dot))), (16, 128))
    spread = spread_ref[...]
    for at in range(0, D, 512):
        cols = slice(at, at + 512)
        norm = (hid_ref[:, cols].astype(F32) * inverse * gain_ref[:, cols]).astype(BF16)
        norm_ref[:, cols] = norm
        rows = jnp.dot(spread, norm, preferred_element_type=F32)
        send_ref[:, :, cols] = rows.reshape(64, 2, 512).astype(BF16)
    for s, out in enumerate((n0_ref, n1_ref, n2_ref, n3_ref)):
        to = lax.rem(c_ref[1] + s, NY)
        for z in range(NZ):
            at = pl.multiple_of((z * NY + to) * 128, 128)
            out[:, z * 128 : (z + 1) * 128] = norm_ref[:, pl.ds(at, 128)]


def settle(c, got, tok, gain, mix_row, spread):
    part = jax.ShapeDtypeStruct((16, 1024), BF16)
    return pl.pallas_call(
        settle_kernel,
        out_shape=(
            jax.ShapeDtypeStruct((16, D), BF16),
            jax.ShapeDtypeStruct((16, 128), F32),
            jax.ShapeDtypeStruct((64, 2, D), BF16),
            part, part, part, part,
        ),
        in_specs=[SMEM] + [VMEM] * 5,
        out_specs=(VMEM,) * 7,
        scratch_shapes=[pltpu.VMEM((16, D), BF16)],
        cost_estimate=pl.CostEstimate(
            flops=2 * 128 * 128 * 4096, bytes_accessed=3 << 20, transcendentals=0
        ),
        name="settle",
    )(c, got, tok, gain, mix_row, spread)


def dense_kernel(c_ref, x0, x1, x2, x3, mine_ref, away_ref, o0, o1, o2, o3):
    c = c_ref[0]
    acc = jnp.zeros((64, 512), F32)
    for z in range(NZ):
        cols = turned_z(c_ref, z)
        x = jnp.concatenate([r[:, cols] for r in (x0, x1, x2, x3)], axis=0)
        own = jnp.where(c == 0, x[:, :64], x[:, 64:])
        off = jnp.where(c == 0, x[:, 64:], x[:, :64])
        for part, ref in ((own, mine_ref), (off, away_ref)):
            w = jnp.concatenate(
                [ref[z, 272 + j * 64 : 336 + j * 64, :] for j in range(4)], axis=1
            )
            acc += jnp.dot(part, w, preferred_element_type=F32)
    for s, out in enumerate((o0, o1, o2, o3)):
        out[...] = acc[s * 16 : (s + 1) * 16].astype(BF16)


def dense_products(c, xs, mine, away):
    part = jax.ShapeDtypeStruct((16, 512), BF16)
    return pl.pallas_call(
        dense_kernel,
        out_shape=(part,) * 4,
        in_specs=[SMEM] + [VMEM] * 6,
        out_specs=(VMEM,) * 4,
        compiler_params=pltpu.CompilerParams(vmem_limit_bytes=LIMIT),
        cost_estimate=pl.CostEstimate(
            flops=2 * 64 * 1024 * 512, bytes_accessed=2 << 20, transcendentals=0
        ),
        name="dense_products",
    )(c, *xs, mine, away)


def dense_down_kernel(c_ref, x0, x1, x2, x3, mine_ref, away_ref, o0, o1, o2, o3):
    c = c_ref[0]
    xs = (x0, x1, x2, x3)
    both = jnp.concatenate([r[:, :128] for r in xs] + [r[:, 128:] for r in xs], axis=0)
    for z in range(NZ):
        w = jnp.concatenate([mine_ref[z, 528:656, :], away_ref[z, 528:656, :]], axis=1)
        tile = both_kinds(c, jnp.dot(both, w, preferred_element_type=F32), 64)
        for s, out in enumerate((o0, o1, o2, o3)):
            out[:, turned_z(c_ref, z)] = tile[s * 16 : (s + 1) * 16]


def dense_down(c, xs, mine, away):
    part = jax.ShapeDtypeStruct((16, 1024), BF16)
    return pl.pallas_call(
        dense_down_kernel,
        out_shape=(part,) * 4,
        in_specs=[SMEM] + [VMEM] * 6,
        out_specs=(VMEM,) * 4,
        compiler_params=pltpu.CompilerParams(vmem_limit_bytes=LIMIT),
        cost_estimate=pl.CostEstimate(
            flops=2 * 64 * 1024 * 512, bytes_accessed=1 << 20, transcendentals=0
        ),
        name="dense_down",
    )(c, *xs, mine, away)


def half_rows(wide):
    lane = lax.broadcasted_iota(jnp.int32, (8, 128), 1)
    turn = pltpu.roll(wide, 64, 1)
    return (
        jnp.where(lane < 64, wide[:8], turn[8:]),
        jnp.where(lane < 64, turn[:8], wide[8:]),
    )


def down_kernel(c_ref, h_ref, w_ref, hid_ref, d0, d1, d2, d3, out_ref):
    res = jnp.dot(h_ref[...], w_ref[...], preferred_element_type=F32)
    lane = lax.broadcasted_iota(jnp.int32, (64, 128), 1)
    for p in range(8):
        cols = slice(p * 128, (p + 1) * 128)
        top, low = res[:64, cols], res[64:, cols]
        out_ref[2 * p, :64] = jnp.where(lane < 64, top, pltpu.roll(low, 64, 1)).astype(BF16)
        out_ref[2 * p + 1, :64] = jnp.where(lane < 64, pltpu.roll(top, 64, 1), low).astype(BF16)
    quarter = lax.broadcasted_iota(jnp.int32, (16, 128), 0) // 4 == c_ref[3]
    for zl in range(2):
        for s, d in enumerate((d0, d1, d2, d3)):
            at = zl * NY + lax.rem(c_ref[1] + s, NY)
            hid = hid_ref[:, pl.ds(pl.multiple_of(at * 128, 128), 128)].astype(F32)
            wide = d[:, zl * 128 : (zl + 1) * 128].astype(F32) + jnp.where(quarter, hid, 0.0)
            for k, half in enumerate(half_rows(wide)):
                out_ref[2 * at + k, 64:] = half.astype(BF16)


def down_for_all(c, expert_hidden, w, hidden, downs):
    return pl.pallas_call(
        down_kernel,
        grid=(4,),
        out_shape=jax.ShapeDtypeStruct((64, 72, 128), BF16),
        in_specs=[
            SMEM,
            pl.BlockSpec((128, 256), lambda i: (0, 0)),
            pl.BlockSpec((256, 1024), lambda i: (0, i)),
            pl.BlockSpec((16, 1024), lambda i: (0, i)),
        ]
        + [pl.BlockSpec((16, 256), lambda i: (0, i))] * 4,
        out_specs=pl.BlockSpec((16, 72, 128), lambda i: (i, 0, 0)),
        compiler_params=pltpu.CompilerParams(vmem_limit_bytes=LIMIT),
        cost_estimate=pl.CostEstimate(
            flops=2 * 128 * 256 * 4096, bytes_accessed=4 << 20, transcendentals=0
        ),
        name="down",
    )(c, expert_hidden, w, hidden, *downs)


def project_kernel(kept, c_ref, tok_ref, gain_ref, q_ref, k_ref, v_ref, o_ref, i_ref, f_ref, *refs):
    got_ref, out, all_ref, x_ref = refs if kept else (None, *refs)
    c = c_ref[0]
    core = c if kept else 1 - c
    y = pl.program_id(0)

    @pl.when(y == 0)
    def _():
        all_ref[...] = jnp.transpose(tok_ref[...])

    gate_rows = jnp.concatenate(
        [jnp.zeros((64, 64), BF16), i_ref[...], f_ref[...], jnp.zeros((56, 64), BF16)], axis=0
    )
    for z in range(NZ):
        at = pl.multiple_of(((z * NY + y) * NC + core) * 16, 16)
        x_ref[z * 16 : (z + 1) * 16, :] = all_ref[pl.ds(at, 16), :]
    wide = x_ref[...].astype(F32)
    scaled = (wide * gain_ref[...].astype(F32)).astype(BF16)
    at = 0
    for w in (q_ref, k_ref, v_ref, o_ref):
        for half in range(0, w.shape[1], 256):
            res = jnp.dot(scaled, w[:, half : half + 256], preferred_element_type=F32)
            cols = slice(at, at + 256)
            if kept:
                res += got_ref[:, cols].astype(F32)
            out[0, :, cols] = res.astype(BF16)
            at += 256
    lane = lax.broadcasted_iota(jnp.int32, (128, 128), 1)
    gates = lax.dot_general(
        scaled, gate_rows, (((1,), (1,)), ((), ())), preferred_element_type=F32
    )
    square = jnp.sum(wide * wide, axis=1, keepdims=True)
    both = jnp.concatenate([wide, jnp.zeros((128, 64), F32)], axis=1)
    last = jnp.where(lane < 64, both, jnp.where(lane == 72, square, gates))
    if not kept:
        out[0, :, 1536:] = last.astype(BF16)
    else:
        other = got_ref[:, 1536:].astype(F32)
        out[0, :, 1536:1664] = (last + other).astype(BF16)
        first = jnp.where(c == 0, last, other)
        second = jnp.where(c == 0, other, last)
        out[0, :, 1664:] = jnp.where(lane < 64, first, pltpu.roll(second, 64, 1)).astype(BF16)


def project(kept, *args):
    whole = lambda *shape: pl.BlockSpec(shape, lambda g: (0,) * len(shape))
    wide = 1792 if kept else 1664
    return pl.pallas_call(
        functools.partial(project_kernel, kept),
        grid=(NY,),
        out_shape=jax.ShapeDtypeStruct((NY, 128, wide), BF16),
        in_specs=[SMEM]
        + [whole(*a.shape) for a in args[1:9]]
        + [pl.BlockSpec((None, 128, 1664), lambda g: (g, 0, 0))] * kept,
        out_specs=pl.BlockSpec((1, 128, wide), lambda g: (g, 0, 0)),
        scratch_shapes=[pltpu.VMEM((1024, 64), BF16), pltpu.VMEM((128, 64), BF16)],
        cost_estimate=pl.CostEstimate(
            flops=2 * 512 * 256 * 1664, bytes_accessed=3 << 20, transcendentals=0
        ),
        name="project_kept" if kept else "project_away",
    )(*args)


def fold_y_kernel(in_ref, out_ref):
    for z in range(NZ):
        rows = slice(z * 16, (z + 1) * 16)
        total = in_ref[0, rows, :1664].astype(F32)
        for y in range(1, NY):
            total += in_ref[y, rows, :1664].astype(F32)
        out_ref[z, :, :1664] = total.astype(BF16)
        for y in range(NY):
            at = 1664 + y * 128
            out_ref[z, :, at : at + 128] = in_ref[y, rows, 1664:]


def fold_y(x):
    return pl.pallas_call(
        fold_y_kernel,
        out_shape=jax.ShapeDtypeStruct((NZ, 16, 2176), BF16),
        in_specs=[VMEM],
        out_specs=VMEM,
        cost_estimate=pl.CostEstimate(
            flops=1 << 20, bytes_accessed=3 << 20, transcendentals=0
        ),
        name="fold_y",
    )(x)


def recur_kernel(
    in_ref, ib_ref, fb_ref, hg_ref, sm_ref, sn_ref, mx_ref,
    heads_ref, tok_ref, nm_ref, nn_ref, nx_ref,
    kt_ref, qt_ref, car_ref, flo_ref, val_ref, out_ref, num_ref,
):
    g = pl.program_id(0)

    @pl.when(g == 0)
    def _():
        total = in_ref[0, :, :1664].astype(F32)
        for z in range(1, NZ):
            total += in_ref[z, :, :1664].astype(F32)
        for z in range(NZ):
            for y in range(NY):
                at, src = (z * NY + y) * 128, 1664 + y * 128
                tok_ref[:, at : at + 128] = in_ref[z, :, src : src + 128]
        inverse = lax.rsqrt(total[:, 1608:1609] / D + EPSILON)
        total = total * inverse
        q = total[:, :256].astype(BF16).astype(F32) * 0.125
        k = total[:, 256:512].astype(BF16).astype(F32)
        for h in range(4):
            cols = slice(512 + h * 128, 640 + h * 128)
            val_ref[h] = total[:, cols].astype(BF16).astype(F32)
        out_ref[...] = total[:, 1024:1536].astype(BF16).astype(F32)
        in_log = SOFT_CAP * jnp.tanh((total[:, 1600:1604] + ib_ref[...]) / SOFT_CAP)
        f = SOFT_CAP * jnp.tanh((total[:, 1604:1608] + fb_ref[...]) / SOFT_CAP)
        forget_log = jnp.minimum(f, 0.0) - jnp.log1p(jnp.exp(-jnp.abs(f)))
        kept = forget_log + mx_ref[...]
        top = jnp.maximum(kept, in_log)
        nx_ref[...] = top
        carried = jnp.exp(kept - top)
        fresh = jnp.exp(in_log - top)
        least = jnp.exp(-top)
        scaled = []
        for h in range(4):
            cols = slice(h * 64, (h + 1) * 64)
            fk = fresh[:, h : h + 1] * k[:, cols]
            scaled.append(fk)
            norm = carried[:, h : h + 1] * sn_ref[:, h, :] + fk
            nn_ref[:, h, :] = norm
            den = jnp.abs(jnp.sum(norm * q[:, cols], axis=1, keepdims=True))
            flo_ref[h] = jnp.broadcast_to(jnp.maximum(den, least[:, h : h + 1]), (16, 128))
            car_ref[h] = jnp.broadcast_to(carried[:, h : h + 1], (16, 128))
        kt = jnp.transpose(jnp.concatenate(scaled, axis=1))
        qt = jnp.transpose(q)
        for i in range(4):
            kt_ref[i] = kt[:, i * 4 : (i + 1) * 4]
            qt_ref[i] = qt[:, i * 4 : (i + 1) * 4]

    for i in range(4):
        b = g * 4 + i
        for h in range(4):
            rows = slice(h * 64, (h + 1) * 64)
            new = (
                car_ref[h, pl.ds(b, 1), :] * sm_ref[i, h]
                + kt_ref[g, rows, i : i + 1] * val_ref[h, pl.ds(b, 1), :]
            )
            nm_ref[i, h] = new
            num_ref[h, pl.ds(b, 1), :] = jnp.sum(
                new * qt_ref[g, rows, i : i + 1], axis=0, keepdims=True
            )

    @pl.when(g == 3)
    def _():
        for h in range(4):
            cols = slice(h * 128, (h + 1) * 128)
            read = num_ref[h] / flo_ref[h]
            mean = jnp.mean(read * read, axis=1, keepdims=True)
            gate = 1.0 / (1.0 + jnp.exp(-out_ref[:, cols]))
            scaled = read * lax.rsqrt(mean + EPSILON) * hg_ref[:, cols].astype(F32)
            heads_ref[:, cols] = (scaled * gate).astype(BF16)


def recur(x, igate_bias, fgate_bias, head_gain, state_matrix, state_norm, state_max):
    whole = lambda *shape: pl.BlockSpec(shape, lambda g: (0,) * len(shape))
    block = pl.BlockSpec((4, 4, 64, 128), lambda g: (g, 0, 0, 0))
    return pl.pallas_call(
        recur_kernel,
        grid=(4,),
        out_shape=(
            jax.ShapeDtypeStruct((16, 512), BF16),
            jax.ShapeDtypeStruct((16, D), BF16),
            jax.ShapeDtypeStruct((16, 4, 64, 128), F32),
            jax.ShapeDtypeStruct((16, 4, 64), F32),
            jax.ShapeDtypeStruct((16, 4), F32),
        ),
        in_specs=[
            whole(NZ, 16, 2176), whole(1, 4), whole(1, 4), whole(1, 512),
            block, whole(16, 4, 64), whole(16, 4),
        ],
        out_specs=(whole(16, 512), whole(16, D), block, whole(16, 4, 64), whole(16, 4)),
        scratch_shapes=[
            pltpu.VMEM((4, 256, 4), F32),
            pltpu.VMEM((4, 256, 4), F32),
            pltpu.VMEM((4, 16, 128), F32),
            pltpu.VMEM((4, 16, 128), F32),
            pltpu.VMEM((4, 16, 128), F32),
            pltpu.VMEM((16, 512), F32),
            pltpu.VMEM((4, 16, 128), F32),
        ],
        cost_estimate=pl.CostEstimate(
            flops=8 << 20, bytes_accessed=5 << 20, transcendentals=1 << 14
        ),
        name="recur",
    )(x, igate_bias[None], fgate_bias[None], head_gain[None], state_matrix, state_norm, state_max)


def rank_kernel(me_ref, routes_ref, weights_ref, target_ref, spread_ref, weight_ref):
    me = me_ref[0]
    expert = lax.broadcasted_iota(jnp.int32, (64, 128), 0)
    a = lax.broadcasted_iota(jnp.int32, (128, 128), 0)
    b = lax.broadcasted_iota(jnp.int32, (128, 128), 1)
    before = jnp.where((a < b) & (a // 16 == b // 16), 1.0, 0.0).astype(BF16)
    weight = jnp.zeros((128, 128), F32)
    for t in range(8):
        cols = slice(t * 128, (t + 1) * 128)
        hits = [expert == routes_ref[j : j + 1, cols] for j in range(4)]
        count = sum(jnp.where(h, 1.0, 0.0) for h in hits)
        earlier = jnp.dot(count.astype(BF16), before, preferred_element_type=F32)
        for j in range(4):
            rank = jnp.sum(jnp.where(hits[j], earlier, 0.0), axis=0, keepdims=True)
            target = routes_ref[j : j + 1, cols] * 2 + rank.astype(jnp.int32)
            target_ref[j : j + 1, cols] = target
            mine = (target == me * 2 + a % 2) & (b // 16 + t * 8 == a // 2)
            weight += jnp.where(mine, weights_ref[j : j + 1, cols], 0.0)
    weight_ref[...] = jnp.broadcast_to(jnp.sum(weight, axis=1, keepdims=True), (128, 128))
    cols = pl.ds(pl.multiple_of((me // 8) * 128, 128), 128)
    named = a == target_ref[0:1, cols]
    for j in range(1, 4):
        named = named | (a == target_ref[j : j + 1, cols])
    lane = lax.broadcasted_iota(jnp.int32, (128, 16), 0)
    row = lax.broadcasted_iota(jnp.int32, (128, 16), 1)
    own = jnp.where(lane == lax.rem(me, 8) * 16 + row, 1.0, 0.0).astype(BF16)
    spread_ref[...] = jnp.dot(
        jnp.where(named, 1.0, 0.0).astype(BF16), own, preferred_element_type=F32
    ).astype(BF16)


def rank_rows(me, routes, weights):
    return pl.pallas_call(
        rank_kernel,
        out_shape=(
            jax.ShapeDtypeStruct((4, 1024), jnp.int32),
            jax.ShapeDtypeStruct((128, 16), BF16),
            jax.ShapeDtypeStruct((128, 128), F32),
        ),
        in_specs=[SMEM, VMEM, VMEM],
        out_specs=(VMEM,) * 3,
        cost_estimate=pl.CostEstimate(flops=1 << 24, bytes_accessed=1 << 20, transcendentals=0),
        name="rank_rows",
    )(me, routes, weights)


def pick_kernel(target_ref, out_ref):
    at = lax.broadcasted_iota(jnp.int32, (128, 128), 0)
    row = lax.broadcasted_iota(jnp.int32, (1, 128), 1)
    for t in range(8):
        cols = slice(t * 128, (t + 1) * 128)
        local = []
        for j in range(4):
            target = target_ref[j : j + 1, cols]
            local.append((target // 2) * 16 + 2 * (row // 16) + target % 2)
        for k in range(8):
            hit = at + k * 128 == local[0]
            for j in range(1, 4):
                hit = hit | (at + k * 128 == local[j])
            out_ref[t, k * 128 : (k + 1) * 128, :] = jnp.where(hit, 1.0, 0.0).astype(BF16)


def picks(target):
    return pl.pallas_call(
        pick_kernel,
        out_shape=jax.ShapeDtypeStruct((8, 1024, 128), BF16),
        in_specs=[VMEM],
        out_specs=VMEM,
        compiler_params=pltpu.CompilerParams(vmem_limit_bytes=LIMIT),
        cost_estimate=pl.CostEstimate(flops=1 << 24, bytes_accessed=2 << 20, transcendentals=0),
        name="picks",
    )(target)


def finish_kernel(c_ref, b0, b1, b2, b3, out_ref):
    x = c_ref[3]
    parts = [r[...].astype(F32) for r in (b0, b1, b2, b3)]
    total = None
    for a in range(NX):
        s = lax.rem(x + (NX - a), NX)
        part = jnp.where(
            s == 0, parts[0], jnp.where(s == 1, parts[1], jnp.where(s == 2, parts[2], parts[3]))
        )
        total = part if total is None else total + part
    turned = jnp.transpose(total)
    out_ref[:, :512] = turned[:64].astype(BF16)
    out_ref[:, 512:] = turned[64:].astype(BF16)


def finish(c, parts):
    return pl.pallas_call(
        finish_kernel,
        out_shape=jax.ShapeDtypeStruct((64, 1024), BF16),
        in_specs=[SMEM] + [VMEM] * 4,
        out_specs=VMEM,
        compiler_params=pltpu.CompilerParams(vmem_limit_bytes=LIMIT),
        cost_estimate=pl.CostEstimate(flops=1 << 20, bytes_accessed=1 << 20, transcendentals=0),
        name="finish",
    )(c, *parts)


def layer(
    tokens,
    mix_gain,
    w_query,
    w_key,
    w_value,
    w_outgate,
    w_igate,
    w_fgate,
    igate_bias,
    fgate_bias,
    head_gain,
    w_mixout,
    state_matrix,
    state_norm,
    state_max,
    ffn_gain,
    dense_mix,
    w_dense_gate,
    w_dense_up,
    w_dense_down,
    routes,
    route_weights,
    w_exp_gate,
    w_exp_up,
    w_exp_down,
):
    me = lax.axis_index(EP)
    c = lax.axis_index("c")
    y, z = lax.axis_index("y"), lax.axis_index("z")
    c_ref = jnp.stack([c, y, z, lax.axis_index("x")]).astype(jnp.int32)
    piece = jnp.concatenate(
        [
            packed(w_mixout),
            jnp.stack([jnp.pad(ffn_gain, (0, 64)), jnp.pad(dense_mix, (0, 64))]),
            jnp.zeros((14, 128), BF16),
            w_dense_gate[:, :128],
            w_dense_gate[:, 128:],
            w_dense_up[:, :128],
            w_dense_up[:, 128:],
            packed(w_dense_down),
        ],
        axis=0,
    )
    operands = (
        c_ref, tokens.T, mix_gain[None], w_query, w_key, w_value, w_outgate, w_igate.T, w_fgate.T
    )
    away = project(False, *operands)
    got = other_core(away)
    folded = project(True, *operands, got)
    folded = exchanged(folded, "y")
    folded = fold_y(folded)
    folded = exchanged(folded, "z")
    heads_out, tok, new_matrix, new_norm, new_max = recur(
        folded, igate_bias, fgate_bias, head_gain, state_matrix, state_norm, state_max
    )
    mine, away = gathered_z(piece)
    extra = jnp.stack([mine[:, 256:258, :64], away[:, 256:258, :64]])
    extra = jnp.where(c == 0, extra, extra[::-1])[:, (z - jnp.arange(NZ)) % NZ]
    extra = extra.transpose(2, 1, 0, 3).reshape(4, 512)
    heads = jnp.concatenate([heads_out, extra, jnp.zeros((4, 512), BF16)], axis=0)
    heads = [heads] + [
        lax.ppermute(heads, "y", [(i, (i + s) % NY) for i in range(NY)]) for s in (1, 2, 3)
    ]
    vectors = jnp.stack([h[16:20] for h in heads])[(y - jnp.arange(NY)) % NY]
    vectors = vectors.reshape(NY, 2, NZ, 128).transpose(1, 2, 0, 3).reshape(2, 1, D)
    vectors = vectors.astype(F32)
    partial = mix(c_ref, heads, mine, away)
    copies = jnp.broadcast_to(partial[:, None], (NY, NX, 16, 1024)).reshape(16, 16, 1024)
    got = exchanged(copies, ("y", "x")).reshape(NY, NX, 16, 1024)
    target, spread, weight = rank_rows(
        jnp.full((1,), me, jnp.int32), routes.T, route_weights.T
    )
    hidden, dense_gate, send, *sides = settle(c_ref, got, tok, vectors[0], vectors[1], spread)
    arrived = exchanged(send, EP).reshape(128, D)
    xs = [sides[0]] + [
        lax.ppermute(sides[s], "y", [(i, (i + s) % NY) for i in range(NY)]) for s in (1, 2, 3)
    ]
    sums = dense_products(c_ref, xs, mine, away)
    parts = [sums[0]] + [
        lax.ppermute(sums[s], "y", [(i, (i - s) % NY) for i in range(NY)]) for s in (1, 2, 3)
    ]
    dense_sum = sum(p.astype(F32) for p in parts)
    dense_hidden = (
        jax.nn.silu(dense_sum[:, :256]) * dense_sum[:, 256:] * dense_gate[:, :1]
    ).astype(BF16)
    units = [dense_hidden] + [
        lax.ppermute(dense_hidden, "y", [(i, (i + s) % NY) for i in range(NY)])
        for s in (1, 2, 3)
    ]
    downs = dense_down(c_ref, units, mine, away)
    downs = [downs[0]] + [
        lax.ppermute(downs[s], "y", [(i, (i - s) % NY) for i in range(NY)]) for s in (1, 2, 3)
    ]
    gate_part = jnp.dot(arrived, w_exp_gate[0], preferred_element_type=F32)
    up_part = jnp.dot(arrived, w_exp_up[0], preferred_element_type=F32)
    expert_hidden = (jax.nn.silu(gate_part) * up_part * weight[:, :1]).astype(BF16)
    returned = down_for_all(c_ref, expert_hidden, w_exp_down[0], hidden, downs)
    returned = exchanged(returned, EP)
    dense_rows = returned[:, 64:].reshape(64, 8, 2, 64).transpose(0, 2, 1, 3).reshape(1024, 64)
    returned = returned[:, :64]
    source = returned.reshape(64, 4, 16, 128).transpose(1, 0, 2, 3).reshape(4, 1024, 128)
    pick = picks(target).reshape(2, 4, 1024, 128)
    halves = jnp.einsum("hgkm,gkn->hgmn", pick, source, preferred_element_type=F32)
    routed = jnp.concatenate(
        [halves[0, :, :, :64].reshape(512, 64), halves[1, :, :, 64:].reshape(512, 64)], axis=0
    )
    branch = packed((routed + dense_rows.astype(F32)).astype(BF16))
    branches = [branch] + [
        lax.ppermute(branch, "x", [(i, (i + s) % NX) for i in range(NX)]) for s in (1, 2, 3)
    ]
    layer_out = finish(c_ref, branches).T
    return (layer_out, new_matrix, new_norm, new_max)


def solution(mesh):
    return jax.shard_map(
        layer,
        mesh=Mesh(mesh.devices.reshape(NZ, NY, NC, NX), ("z", "y", "c", "x")),
        in_specs=(
            P(None, EP),
            P(EP),
            P(EP, "x"),
            P(EP, "x"),
            P(EP, "x"),
            P(EP, "x"),
            P(EP, "x"),
            P(EP, "x"),
            P("x"),
            P("x"),
            P("x"),
            P("x", EP),
            P(EP, "x", None, None),
            P(EP, "x", None),
            P(EP, "x"),
            P(EP),
            P(EP),
            P(EP, "x"),
            P(EP, "x"),
            P("x", EP),
            P(),
            P(),
            P(EP, None, "x"),
            P(EP, None, "x"),
            P(EP, "x", None),
        ),
        out_specs=(P(None, EP), P(EP, "x", None, None), P(EP, "x", None), P(EP, "x")),
        check_vma=False,
    )
```

```python
import functools

import jax
import jax.numpy as jnp
from jax import lax
from jax.experimental import pallas as pl
from jax.experimental.pallas import tpu as pltpu
from jax.sharding import Mesh
from jax.sharding import PartitionSpec as P


D = 4096


EPSILON = 1e-06
SOFT_CAP = 15.0
NZ, NY, NC, NX = 8, 4, 2, 4
EP = ("z", "y", "c")
F32, BF16 = jnp.float32, jnp.bfloat16
LIMIT = 16 << 20


def exchanged(x, axis):
    return lax.all_to_all(x, axis, split_axis=0, concat_axis=0, tiled=True)


def other_core(x):
    return lax.ppermute(x, "c", [(0, 1), (1, 0)])


def stacked_kernel(*refs):
    for i in range(NZ):
        refs[-1][i] = refs[i][...]


def gathered_z(x):
    pieces = [x] + [None] * (NZ - 1)
    up, down = x, x
    for s in range(1, NZ // 2 + 1):
        up = lax.ppermute(up, "z", [(i, (i + 1) % NZ) for i in range(NZ)])
        pieces[s] = up
        if s < NZ // 2:
            down = lax.ppermute(down, "z", [(i, (i - 1) % NZ) for i in range(NZ)])
            pieces[NZ - s] = down
    zs = pl.pallas_call(
        stacked_kernel,
        out_shape=jax.ShapeDtypeStruct((NZ, *x.shape), x.dtype),
        in_specs=[VMEM] * NZ,
        out_specs=VMEM,
        cost_estimate=pl.CostEstimate(flops=1 << 20, bytes_accessed=2 << 20, transcendentals=0),
        name="stacked",
    )(*pieces)
    return zs, other_core(zs)


def packed(x):
    h = x.shape[0] // 2
    return jnp.concatenate([x[:h], x[h:]], axis=1)


def turned_z(place_ref, z):
    az = lax.rem(place_ref[2] + (NZ - z), NZ)
    return pl.ds(pl.multiple_of(az * 128, 128), 128)


def both_kinds(c, r, n):
    lane = lax.broadcasted_iota(jnp.int32, (n, 128), 1)
    res = []
    for k in range(2):
        top, low = r[:n, k * 128 : (k + 1) * 128], r[n:, k * 128 : (k + 1) * 128]
        res.append((top + pltpu.roll(low, 64, 1), pltpu.roll(top, 64, 1) + low))
    first = jnp.where(c == 0, res[0][0], res[1][0])
    second = jnp.where(c == 0, res[1][1], res[0][1])
    return jnp.where(lane < 64, first, second)


def mix_kernel(c_ref, x0, x1, x2, x3, tok_ref, mine_ref, away_ref, out_ref):
    c = c_ref[0]
    xs = (x0, x1, x2, x3)
    both = jnp.concatenate([r[:16, :256] for r in xs] + [r[:16, 256:] for r in xs], axis=0)
    for z in range(NZ):
        w = jnp.concatenate([mine_ref[z, :256, :], away_ref[z, :256, :]], axis=1)
        tile = both_kinds(c, jnp.dot(both, w, preferred_element_type=F32), 64)
        tok = tok_ref[:, turned_z(c_ref, z)].astype(F32)
        for s in range(NY):
            to = lax.rem(c_ref[1] + (NY - s), NY)
            rows = tile[s * 16 : (s + 1) * 16] + jnp.where(to == c_ref[3], tok, 0.0)
            out_ref[to, :, turned_z(c_ref, z)] = rows.astype(BF16)


VMEM = pl.BlockSpec(memory_space=pltpu.VMEM)
SMEM = pl.BlockSpec(memory_space=pltpu.SMEM)


def mix(c, heads, tok, mine, away):
    return pl.pallas_call(
        mix_kernel,
        out_shape=jax.ShapeDtypeStruct((NY, 16, 1024), BF16),
        in_specs=[SMEM] + [VMEM] * 7,
        out_specs=VMEM,
        compiler_params=pltpu.CompilerParams(vmem_limit_bytes=LIMIT),
        cost_estimate=pl.CostEstimate(
            flops=2 * 128 * 256 * 128 * 16, bytes_accessed=2 << 20, transcendentals=0
        ),
        name="mix",
    )(c, *heads, tok, mine, away)


def settle_kernel(
    c_ref, got_ref, gain_ref, mix_ref, spread_ref,
    hid_ref, gate_ref, send_ref, n0_ref, n1_ref, n2_ref, n3_ref, norm_ref,
):
    square = jnp.zeros((16, 1), F32)
    dot = jnp.zeros((16, 1), F32)
    for y in range(NY):
        total = got_ref[y, 0].astype(F32)
        for x in range(1, NX):
            total += got_ref[y, x].astype(F32)
        for z in range(NZ):
            at = (z * NY + y) * 128
            cols = slice(at, at + 128)
            hid = total[:, z * 128 : (z + 1) * 128].astype(BF16)
            hid_ref[:, cols] = hid
            wide = hid.astype(F32)
            square += jnp.sum(wide * wide, axis=1, keepdims=True)
            dot += jnp.sum(wide * gain_ref[:, cols] * mix_ref[:, cols], axis=1, keepdims=True)
    inverse = lax.rsqrt(square / D + EPSILON)
    gate_ref[...] = jnp.broadcast_to(1.0 / (1.0 + jnp.exp(-(inverse * dot))), (16, 128))
    spread = spread_ref[...]
    for at in range(0, D, 512):
        cols = slice(at, at + 512)
        norm = (hid_ref[:, cols].astype(F32) * inverse * gain_ref[:, cols]).astype(BF16)
        norm_ref[:, cols] = norm
        rows = jnp.dot(spread, norm, preferred_element_type=F32)
        send_ref[:, :, cols] = rows.reshape(64, 2, 512).astype(BF16)
    for s, out in enumerate((n0_ref, n1_ref, n2_ref, n3_ref)):
        to = lax.rem(c_ref[1] + s, NY)
        for z in range(NZ):
            at = pl.multiple_of((z * NY + to) * 128, 128)
            out[:, z * 128 : (z + 1) * 128] = norm_ref[:, pl.ds(at, 128)]


def settle(c, got, gain, mix_row, spread):
    part = jax.ShapeDtypeStruct((16, 1024), BF16)
    return pl.pallas_call(
        settle_kernel,
        out_shape=(
            jax.ShapeDtypeStruct((16, D), BF16),
            jax.ShapeDtypeStruct((16, 128), F32),
            jax.ShapeDtypeStruct((64, 2, D), BF16),
            part, part, part, part,
        ),
        in_specs=[SMEM] + [VMEM] * 4,
        out_specs=(VMEM,) * 7,
        scratch_shapes=[pltpu.VMEM((16, D), BF16)],
        cost_estimate=pl.CostEstimate(
            flops=2 * 128 * 128 * 4096, bytes_accessed=3 << 20, transcendentals=0
        ),
        name="settle",
    )(c, got, gain, mix_row, spread)


def dense_kernel(c_ref, x0, x1, x2, x3, mine_ref, away_ref, out_ref):
    c = c_ref[0]
    acc = jnp.zeros((64, 512), F32)
    for z in range(NZ):
        cols = turned_z(c_ref, z)
        x = jnp.concatenate([r[:, cols] for r in (x0, x1, x2, x3)], axis=0)
        own = jnp.where(c == 0, x[:, :64], x[:, 64:])
        off = jnp.where(c == 0, x[:, 64:], x[:, :64])
        for part, ref in ((own, mine_ref), (off, away_ref)):
            w = jnp.concatenate(
                [ref[z, 272 + j * 64 : 336 + j * 64, :] for j in range(4)], axis=1
            )
            acc += jnp.dot(part, w, preferred_element_type=F32)
    out_ref[...] = acc.astype(BF16)


def dense_products(c, xs, mine, away):
    return pl.pallas_call(
        dense_kernel,
        out_shape=jax.ShapeDtypeStruct((64, 512), BF16),
        in_specs=[SMEM] + [VMEM] * 6,
        out_specs=VMEM,
        compiler_params=pltpu.CompilerParams(vmem_limit_bytes=LIMIT),
        cost_estimate=pl.CostEstimate(
            flops=2 * 64 * 1024 * 512, bytes_accessed=2 << 20, transcendentals=0
        ),
        name="dense_products",
    )(c, *xs, mine, away)


def dense_down_kernel(c_ref, x0, x1, x2, x3, mine_ref, away_ref, o0, o1, o2, o3):
    c = c_ref[0]
    xs = (x0, x1, x2, x3)
    units = []
    for s in range(NY):
        total = jnp.zeros((16, 512), F32)
        for k in range(NY):
            j = (s - k) % NY
            total += xs[k][j * 16 : (j + 1) * 16, :].astype(F32)
        gate = total[:, :256]
        units.append((gate / (1.0 + jnp.exp(-gate)) * total[:, 256:]).astype(BF16))
    both = jnp.concatenate([u[:, :128] for u in units] + [u[:, 128:] for u in units], axis=0)
    for z in range(NZ):
        w = jnp.concatenate([mine_ref[z, 528:656, :], away_ref[z, 528:656, :]], axis=1)
        tile = both_kinds(c, jnp.dot(both, w, preferred_element_type=F32), 64)
        for s, out in enumerate((o0, o1, o2, o3)):
            out[:, turned_z(c_ref, z)] = tile[s * 16 : (s + 1) * 16].astype(BF16)


def dense_down(c, xs, mine, away):
    part = jax.ShapeDtypeStruct((16, 1024), BF16)
    return pl.pallas_call(
        dense_down_kernel,
        out_shape=(part,) * 4,
        in_specs=[SMEM] + [VMEM] * 6,
        out_specs=(VMEM,) * 4,
        compiler_params=pltpu.CompilerParams(vmem_limit_bytes=LIMIT),
        cost_estimate=pl.CostEstimate(
            flops=2 * 64 * 1024 * 512, bytes_accessed=1 << 20, transcendentals=0
        ),
        name="dense_down",
    )(c, *xs, mine, away)


def half_rows(wide):
    lane = lax.broadcasted_iota(jnp.int32, (8, 128), 1)
    turn = pltpu.roll(wide, 64, 1)
    return (
        jnp.where(lane < 64, wide[:8], turn[8:]),
        jnp.where(lane < 64, turn[:8], wide[8:]),
    )


def down_kernel(c_ref, h_ref, w_ref, hid_ref, gate_ref, d0, d1, d2, d3, out_ref):
    res = jnp.dot(h_ref[...], w_ref[...], preferred_element_type=F32)
    lane = lax.broadcasted_iota(jnp.int32, (64, 128), 1)
    for p in range(8):
        cols = slice(p * 128, (p + 1) * 128)
        top, low = res[:64, cols], res[64:, cols]
        out_ref[2 * p, :64] = jnp.where(lane < 64, top, pltpu.roll(low, 64, 1)).astype(BF16)
        out_ref[2 * p + 1, :64] = jnp.where(lane < 64, pltpu.roll(top, 64, 1), low).astype(BF16)
    quarter = lax.broadcasted_iota(jnp.int32, (16, 128), 0) // 4 == c_ref[3]
    for zl in range(2):
        for s, d in enumerate((d0, d1, d2, d3)):
            at = zl * NY + lax.rem(c_ref[1] + s, NY)
            hid = hid_ref[:, pl.ds(pl.multiple_of(at * 128, 128), 128)].astype(F32)
            dense = d[:, zl * 128 : (zl + 1) * 128].astype(F32) * gate_ref[...]
            wide = dense + jnp.where(quarter, hid, 0.0)
            for k, half in enumerate(half_rows(wide)):
                out_ref[2 * at + k, 64:] = half.astype(BF16)


def down_for_all(c, expert_hidden, w, hidden, gate, downs):
    return pl.pallas_call(
        down_kernel,
        grid=(4,),
        out_shape=jax.ShapeDtypeStruct((64, 72, 128), BF16),
        in_specs=[
            SMEM,
            pl.BlockSpec((128, 256), lambda i: (0, 0)),
            pl.BlockSpec((256, 1024), lambda i: (0, i)),
            pl.BlockSpec((16, 1024), lambda i: (0, i)),
            pl.BlockSpec((16, 128), lambda i: (0, 0)),
        ]
        + [pl.BlockSpec((16, 256), lambda i: (0, i))] * 4,
        out_specs=pl.BlockSpec((16, 72, 128), lambda i: (i, 0, 0)),
        compiler_params=pltpu.CompilerParams(vmem_limit_bytes=LIMIT),
        cost_estimate=pl.CostEstimate(
            flops=2 * 128 * 256 * 4096, bytes_accessed=4 << 20, transcendentals=0
        ),
        name="down",
    )(c, expert_hidden, w, hidden, gate, *downs)


def project_kernel(kept, c_ref, tok_ref, gain_ref, q_ref, k_ref, v_ref, o_ref, i_ref, f_ref, *refs):
    got_ref, out, tile_ref, all_ref, x_ref = refs if kept else (None, refs[0], None, *refs[1:])
    c = c_ref[0]
    core = c if kept else 1 - c
    y = pl.program_id(0)

    @pl.when(y == 0)
    def _():
        all_ref[...] = jnp.transpose(tok_ref[...])

    gate_rows = jnp.concatenate(
        [jnp.zeros((64, 64), BF16), i_ref[...], f_ref[...], jnp.zeros((56, 64), BF16)], axis=0
    )
    for z in range(NZ):
        at = pl.multiple_of(((z * NY + y) * NC + core) * 16, 16)
        x_ref[z * 16 : (z + 1) * 16, :] = all_ref[pl.ds(at, 16), :]
    wide = x_ref[...].astype(F32)
    scaled = (wide * gain_ref[...].astype(F32)).astype(BF16)
    at = 0
    for w in (q_ref, k_ref, v_ref, o_ref):
        for half in range(0, w.shape[1], 256):
            res = jnp.dot(scaled, w[:, half : half + 256], preferred_element_type=F32)
            cols = slice(at, at + 256)
            if kept:
                res += got_ref[:, cols].astype(F32)
            out[0, :, cols] = res.astype(BF16)
            at += 256
    lane = lax.broadcasted_iota(jnp.int32, (128, 128), 1)
    gates = lax.dot_general(
        scaled, gate_rows, (((1,), (1,)), ((), ())), preferred_element_type=F32
    )
    square = jnp.sum(wide * wide, axis=1, keepdims=True)
    both = jnp.concatenate([wide, jnp.zeros((128, 64), F32)], axis=1)
    last = jnp.where(lane < 64, both, jnp.where(lane == 72, square, gates))
    if not kept:
        out[0, :, 1536:] = last.astype(BF16)
    else:
        other = got_ref[:, 1536:].astype(F32)
        out[0, :, 1536:1664] = (last + other).astype(BF16)

        @pl.when(y == c_ref[3])
        def _():
            first = jnp.where(c == 0, last, other)
            second = jnp.where(c == 0, other, last)
            tile_ref[...] = jnp.where(lane < 64, first, pltpu.roll(second, 64, 1)).astype(BF16)


def project(kept, *args):
    whole = lambda *shape: pl.BlockSpec(shape, lambda g: (0,) * len(shape))
    return pl.pallas_call(
        functools.partial(project_kernel, kept),
        grid=(NY,),
        out_shape=(jax.ShapeDtypeStruct((NY, 128, 1664), BF16),)
        + (jax.ShapeDtypeStruct((128, 128), BF16),) * kept,
        in_specs=[SMEM]
        + [whole(*a.shape) for a in args[1:9]]
        + [pl.BlockSpec((None, 128, 1664), lambda g: (g, 0, 0))] * kept,
        out_specs=(pl.BlockSpec((1, 128, 1664), lambda g: (g, 0, 0)),) + (whole(128, 128),) * kept,
        scratch_shapes=[pltpu.VMEM((1024, 64), BF16), pltpu.VMEM((128, 64), BF16)],
        cost_estimate=pl.CostEstimate(
            flops=2 * 512 * 256 * 1664, bytes_accessed=3 << 20, transcendentals=0
        ),
        name="project_kept" if kept else "project_away",
    )(*args)


def fold_y_kernel(in_ref, tile_ref, out_ref):
    for z in range(NZ):
        rows = slice(z * 16, (z + 1) * 16)
        total = in_ref[0, rows, :].astype(F32)
        for y in range(1, NY):
            total += in_ref[y, rows, :].astype(F32)
        out_ref[z, :, :1664] = total.astype(BF16)
        out_ref[z, :, 1664:] = tile_ref[rows, :]


def fold_y(x, tile):
    return pl.pallas_call(
        fold_y_kernel,
        out_shape=jax.ShapeDtypeStruct((NZ, 16, 1792), BF16),
        in_specs=[VMEM, VMEM],
        out_specs=VMEM,
        cost_estimate=pl.CostEstimate(
            flops=1 << 20, bytes_accessed=3 << 20, transcendentals=0
        ),
        name="fold_y",
    )(x, tile)


def recur_kernel(
    in_ref, ib_ref, fb_ref, hg_ref, sm_ref, sn_ref, mx_ref,
    heads_ref, tok_ref, nm_ref, nn_ref, nx_ref,
    kt_ref, qt_ref, car_ref, flo_ref, val_ref, out_ref, num_ref,
):
    g = pl.program_id(0)

    @pl.when(g == 0)
    def _():
        total = in_ref[0, :, :1664].astype(F32)
        for z in range(1, NZ):
            total += in_ref[z, :, :1664].astype(F32)
        for z in range(NZ):
            tok_ref[:, z * 128 : (z + 1) * 128] = in_ref[z, :, 1664:]
        inverse = lax.rsqrt(total[:, 1608:1609] / D + EPSILON)
        total = total * inverse
        q = total[:, :256].astype(BF16).astype(F32) * 0.125
        k = total[:, 256:512].astype(BF16).astype(F32)
        for h in range(4):
            cols = slice(512 + h * 128, 640 + h * 128)
            val_ref[h] = total[:, cols].astype(BF16).astype(F32)
        out_ref[...] = total[:, 1024:1536].astype(BF16).astype(F32)
        in_log = SOFT_CAP * jnp.tanh((total[:, 1600:1604] + ib_ref[...]) / SOFT_CAP)
        f = SOFT_CAP * jnp.tanh((total[:, 1604:1608] + fb_ref[...]) / SOFT_CAP)
        forget_log = jnp.minimum(f, 0.0) - jnp.log1p(jnp.exp(-jnp.abs(f)))
        kept = forget_log + mx_ref[...]
        top = jnp.maximum(kept, in_log)
        nx_ref[...] = top
        carried = jnp.exp(kept - top)
        fresh = jnp.exp(in_log - top)
        least = jnp.exp(-top)
        scaled = []
        for h in range(4):
            cols = slice(h * 64, (h + 1) * 64)
            fk = fresh[:, h : h + 1] * k[:, cols]
            scaled.append(fk)
            norm = carried[:, h : h + 1] * sn_ref[:, h, :] + fk
            nn_ref[:, h, :] = norm
            den = jnp.abs(jnp.sum(norm * q[:, cols], axis=1, keepdims=True))
            flo_ref[h] = jnp.broadcast_to(jnp.maximum(den, least[:, h : h + 1]), (16, 128))
            car_ref[h] = jnp.broadcast_to(carried[:, h : h + 1], (16, 128))
        kt = jnp.transpose(jnp.concatenate(scaled, axis=1))
        qt = jnp.transpose(q)
        for i in range(4):
            kt_ref[i] = kt[:, i * 4 : (i + 1) * 4]
            qt_ref[i] = qt[:, i * 4 : (i + 1) * 4]

    for i in range(4):
        b = g * 4 + i
        for h in range(4):
            rows = slice(h * 64, (h + 1) * 64)
            new = (
                car_ref[h, pl.ds(b, 1), :] * sm_ref[i, h]
                + kt_ref[g, rows, i : i + 1] * val_ref[h, pl.ds(b, 1), :]
            )
            nm_ref[i, h] = new
            num_ref[h, pl.ds(b, 1), :] = jnp.sum(
                new * qt_ref[g, rows, i : i + 1], axis=0, keepdims=True
            )

    @pl.when(g == 3)
    def _():
        for h in range(4):
            cols = slice(h * 128, (h + 1) * 128)
            read = num_ref[h] / flo_ref[h]
            mean = jnp.mean(read * read, axis=1, keepdims=True)
            gate = 1.0 / (1.0 + jnp.exp(-out_ref[:, cols]))
            scaled = read * lax.rsqrt(mean + EPSILON) * hg_ref[:, cols].astype(F32)
            heads_ref[:, cols] = (scaled * gate).astype(BF16)


def recur(x, igate_bias, fgate_bias, head_gain, state_matrix, state_norm, state_max):
    whole = lambda *shape: pl.BlockSpec(shape, lambda g: (0,) * len(shape))
    block = pl.BlockSpec((4, 4, 64, 128), lambda g: (g, 0, 0, 0))
    return pl.pallas_call(
        recur_kernel,
        grid=(4,),
        out_shape=(
            jax.ShapeDtypeStruct((16, 512), BF16),
            jax.ShapeDtypeStruct((16, 1024), BF16),
            jax.ShapeDtypeStruct((16, 4, 64, 128), F32),
            jax.ShapeDtypeStruct((16, 4, 64), F32),
            jax.ShapeDtypeStruct((16, 4), F32),
        ),
        in_specs=[
            whole(NZ, 16, 1792), whole(1, 4), whole(1, 4), whole(1, 512),
            block, whole(16, 4, 64), whole(16, 4),
        ],
        out_specs=(whole(16, 512), whole(16, 1024), block, whole(16, 4, 64), whole(16, 4)),
        scratch_shapes=[
            pltpu.VMEM((4, 256, 4), F32),
            pltpu.VMEM((4, 256, 4), F32),
            pltpu.VMEM((4, 16, 128), F32),
            pltpu.VMEM((4, 16, 128), F32),
            pltpu.VMEM((4, 16, 128), F32),
            pltpu.VMEM((16, 512), F32),
            pltpu.VMEM((4, 16, 128), F32),
        ],
        cost_estimate=pl.CostEstimate(
            flops=8 << 20, bytes_accessed=5 << 20, transcendentals=1 << 14
        ),
        name="recur",
    )(x, igate_bias[None], fgate_bias[None], head_gain[None], state_matrix, state_norm, state_max)


def rank_kernel(me_ref, routes_ref, weights_ref, target_ref, spread_ref, weight_ref):
    me = me_ref[0]
    expert = lax.broadcasted_iota(jnp.int32, (64, 128), 0)
    a = lax.broadcasted_iota(jnp.int32, (128, 128), 0)
    b = lax.broadcasted_iota(jnp.int32, (128, 128), 1)
    before = jnp.where((a < b) & (a // 16 == b // 16), 1.0, 0.0).astype(BF16)
    weight = jnp.zeros((128, 128), F32)
    for t in range(8):
        cols = slice(t * 128, (t + 1) * 128)
        hits = [expert == routes_ref[j : j + 1, cols] for j in range(4)]
        count = sum(jnp.where(h, 1.0, 0.0) for h in hits)
        earlier = jnp.dot(count.astype(BF16), before, preferred_element_type=F32)
        for j in range(4):
            rank = jnp.sum(jnp.where(hits[j], earlier, 0.0), axis=0, keepdims=True)
            target = routes_ref[j : j + 1, cols] * 2 + rank.astype(jnp.int32)
            target_ref[j : j + 1, cols] = target
            mine = (target == me * 2 + a % 2) & (b // 16 + t * 8 == a // 2)
            weight += jnp.where(mine, weights_ref[j : j + 1, cols], 0.0)
    weight_ref[...] = jnp.broadcast_to(jnp.sum(weight, axis=1, keepdims=True), (128, 128))
    cols = pl.ds(pl.multiple_of((me // 8) * 128, 128), 128)
    named = a == target_ref[0:1, cols]
    for j in range(1, 4):
        named = named | (a == target_ref[j : j + 1, cols])
    lane = lax.broadcasted_iota(jnp.int32, (128, 16), 0)
    row = lax.broadcasted_iota(jnp.int32, (128, 16), 1)
    own = jnp.where(lane == lax.rem(me, 8) * 16 + row, 1.0, 0.0).astype(BF16)
    spread_ref[...] = jnp.dot(
        jnp.where(named, 1.0, 0.0).astype(BF16), own, preferred_element_type=F32
    ).astype(BF16)


def rank_rows(me, routes, weights):
    return pl.pallas_call(
        rank_kernel,
        out_shape=(
            jax.ShapeDtypeStruct((4, 1024), jnp.int32),
            jax.ShapeDtypeStruct((128, 16), BF16),
            jax.ShapeDtypeStruct((128, 128), F32),
        ),
        in_specs=[SMEM, VMEM, VMEM],
        out_specs=(VMEM,) * 3,
        cost_estimate=pl.CostEstimate(flops=1 << 24, bytes_accessed=1 << 20, transcendentals=0),
        name="rank_rows",
    )(me, routes, weights)


def pick_kernel(target_ref, out_ref):
    at = lax.broadcasted_iota(jnp.int32, (128, 128), 0)
    row = lax.broadcasted_iota(jnp.int32, (1, 128), 1)
    for t in range(8):
        cols = slice(t * 128, (t + 1) * 128)
        local = []
        for j in range(4):
            target = target_ref[j : j + 1, cols]
            local.append((target // 2) * 16 + 2 * (row // 16) + target % 2)
        for k in range(8):
            hit = at + k * 128 == local[0]
            for j in range(1, 4):
                hit = hit | (at + k * 128 == local[j])
            out_ref[t, k * 128 : (k + 1) * 128, :] = jnp.where(hit, 1.0, 0.0).astype(BF16)


def picks(target):
    return pl.pallas_call(
        pick_kernel,
        out_shape=jax.ShapeDtypeStruct((8, 1024, 128), BF16),
        in_specs=[VMEM],
        out_specs=VMEM,
        compiler_params=pltpu.CompilerParams(vmem_limit_bytes=LIMIT),
        cost_estimate=pl.CostEstimate(flops=1 << 24, bytes_accessed=2 << 20, transcendentals=0),
        name="picks",
    )(target)


def combine_kernel(got_ref, pick_ref, out_ref):
    lane = lax.broadcasted_iota(jnp.int32, (128, 128), 1)
    lane8 = lax.broadcasted_iota(jnp.int32, (8, 128), 1)
    for g in range(4):
        source = got_ref[:, g * 16 : (g + 1) * 16, :].reshape(1024, 128)
        first, second = (
            lax.dot_general(
                pick_ref[h * 4 + g], source, (((0,), (0,)), ((), ())), preferred_element_type=F32
            )
            for h in range(2)
        )
        rows = []
        for b in range(g * 8, g * 8 + 8):
            left = got_ref[b, 64:, :].astype(F32)
            right = got_ref[b + 32, 64:, :].astype(F32)
            rows.append(jnp.where(lane8 < 64, left, pltpu.roll(right, 64, 1)))
            rows.append(jnp.where(lane8 < 64, pltpu.roll(left, 64, 1), right))
        routed = jnp.where(lane < 64, first, second)
        out_ref[g * 128 : (g + 1) * 128, :] = (routed + jnp.concatenate(rows, axis=0)).astype(BF16)


def combine(returned, pick):
    return pl.pallas_call(
        combine_kernel,
        out_shape=jax.ShapeDtypeStruct((512, 128), BF16),
        in_specs=[VMEM, VMEM],
        out_specs=VMEM,
        compiler_params=pltpu.CompilerParams(vmem_limit_bytes=LIMIT),
        cost_estimate=pl.CostEstimate(flops=1 << 28, bytes_accessed=3 << 20, transcendentals=0),
        name="combine",
    )(returned, pick)


def finish_kernel(c_ref, b0, b1, b2, b3, out_ref):
    x = c_ref[3]
    parts = [r[...].astype(F32) for r in (b0, b1, b2, b3)]
    total = None
    for a in range(NX):
        s = lax.rem(x + (NX - a), NX)
        part = jnp.where(
            s == 0, parts[0], jnp.where(s == 1, parts[1], jnp.where(s == 2, parts[2], parts[3]))
        )
        total = part if total is None else total + part
    turned = jnp.transpose(total)
    out_ref[:, :512] = turned[:64].astype(BF16)
    out_ref[:, 512:] = turned[64:].astype(BF16)


def finish(c, parts):
    return pl.pallas_call(
        finish_kernel,
        out_shape=jax.ShapeDtypeStruct((64, 1024), BF16),
        in_specs=[SMEM] + [VMEM] * 4,
        out_specs=VMEM,
        compiler_params=pltpu.CompilerParams(vmem_limit_bytes=LIMIT),
        cost_estimate=pl.CostEstimate(flops=1 << 20, bytes_accessed=1 << 20, transcendentals=0),
        name="finish",
    )(c, *parts)


def layer(
    tokens,
    mix_gain,
    w_query,
    w_key,
    w_value,
    w_outgate,
    w_igate,
    w_fgate,
    igate_bias,
    fgate_bias,
    head_gain,
    w_mixout,
    state_matrix,
    state_norm,
    state_max,
    ffn_gain,
    dense_mix,
    w_dense_gate,
    w_dense_up,
    w_dense_down,
    routes,
    route_weights,
    w_exp_gate,
    w_exp_up,
    w_exp_down,
):
    me = lax.axis_index(EP)
    c = lax.axis_index("c")
    y, z = lax.axis_index("y"), lax.axis_index("z")
    c_ref = jnp.stack([c, y, z, lax.axis_index("x")]).astype(jnp.int32)
    piece = jnp.concatenate(
        [
            packed(w_mixout),
            jnp.stack([jnp.pad(ffn_gain, (0, 64)), jnp.pad(dense_mix, (0, 64))]),
            jnp.zeros((14, 128), BF16),
            w_dense_gate[:, :128],
            w_dense_gate[:, 128:],
            w_dense_up[:, :128],
            w_dense_up[:, 128:],
            packed(w_dense_down),
        ],
        axis=0,
    )
    operands = (
        c_ref, tokens.T, mix_gain[None], w_query, w_key, w_value, w_outgate, w_igate.T, w_fgate.T
    )
    (away,) = project(False, *operands)
    got = other_core(away)
    folded, tile = project(True, *operands, got)
    folded = exchanged(folded, "y")
    folded = fold_y(folded, tile)
    folded = exchanged(folded, "z")
    heads_out, tok, new_matrix, new_norm, new_max = recur(
        folded, igate_bias, fgate_bias, head_gain, state_matrix, state_norm, state_max
    )
    mine, away = gathered_z(piece)
    extra = jnp.stack([mine[:, 256:258, :64], away[:, 256:258, :64]])
    extra = jnp.where(c == 0, extra, extra[::-1])[:, (z - jnp.arange(NZ)) % NZ]
    extra = extra.transpose(2, 1, 0, 3).reshape(4, 512)
    heads = jnp.concatenate([heads_out, extra, jnp.zeros((4, 512), BF16)], axis=0)
    heads = [heads] + [
        lax.ppermute(heads, "y", [(i, (i + s) % NY) for i in range(NY)]) for s in (1, 2, 3)
    ]
    vectors = jnp.stack([h[16:20] for h in heads])[(y - jnp.arange(NY)) % NY]
    vectors = vectors.reshape(NY, 2, NZ, 128).transpose(1, 2, 0, 3).reshape(2, 1, D)
    vectors = vectors.astype(F32)
    partial = mix(c_ref, heads, tok, mine, away)
    copies = jnp.broadcast_to(partial[:, None], (NY, NX, 16, 1024)).reshape(16, 16, 1024)
    got = exchanged(copies, ("y", "x")).reshape(NY, NX, 16, 1024)
    target, spread, weight = rank_rows(
        jnp.full((1,), me, jnp.int32), routes.T, route_weights.T
    )
    hidden, dense_gate, send, *sides = settle(c_ref, got, vectors[0], vectors[1], spread)
    arrived = exchanged(send, EP).reshape(128, D)
    xs = [sides[0]] + [
        lax.ppermute(sides[s], "y", [(i, (i + s) % NY) for i in range(NY)]) for s in (1, 2, 3)
    ]
    sums = dense_products(c_ref, xs, mine, away)
    sums = [sums] + [
        lax.ppermute(sums, "y", [(i, (i + s) % NY) for i in range(NY)]) for s in (1, 2, 3)
    ]
    downs = dense_down(c_ref, sums, mine, away)
    downs = [downs[0]] + [
        lax.ppermute(downs[s], "y", [(i, (i - s) % NY) for i in range(NY)]) for s in (1, 2, 3)
    ]
    gate_part = jnp.dot(arrived, w_exp_gate[0], preferred_element_type=F32)
    up_part = jnp.dot(arrived, w_exp_up[0], preferred_element_type=F32)
    expert_hidden = (jax.nn.silu(gate_part) * up_part * weight[:, :1]).astype(BF16)
    returned = down_for_all(c_ref, expert_hidden, w_exp_down[0], hidden, dense_gate, downs)
    returned = exchanged(returned, EP)
    branch = combine(returned, picks(target))
    branches = [branch] + [
        lax.ppermute(branch, "x", [(i, (i + s) % NX) for i in range(NX)]) for s in (1, 2, 3)
    ]
    layer_out = finish(c_ref, branches).T
    return (layer_out, new_matrix, new_norm, new_max)


def solution(mesh):
    return jax.shard_map(
        layer,
        mesh=Mesh(mesh.devices.reshape(NZ, NY, NC, NX), ("z", "y", "c", "x")),
        in_specs=(
            P(None, EP),
            P(EP),
            P(EP, "x"),
            P(EP, "x"),
            P(EP, "x"),
            P(EP, "x"),
            P(EP, "x"),
            P(EP, "x"),
            P("x"),
            P("x"),
            P("x"),
            P("x", EP),
            P(EP, "x", None, None),
            P(EP, "x", None),
            P(EP, "x"),
            P(EP),
            P(EP),
            P(EP, "x"),
            P(EP, "x"),
            P("x", EP),
            P(),
            P(),
            P(EP, None, "x"),
            P(EP, None, "x"),
            P(EP, "x", None),
        ),
        out_specs=(P(None, EP), P(EP, "x", None, None), P(EP, "x", None), P(EP, "x")),
        check_vma=False,
    )
```

```python
import functools

import jax
import jax.numpy as jnp
from jax import lax
from jax.experimental import pallas as pl
from jax.experimental.pallas import tpu as pltpu
from jax.sharding import Mesh
from jax.sharding import PartitionSpec as P


D = 4096


EPSILON = 1e-06
SOFT_CAP = 15.0
NZ, NY, NC, NX = 8, 4, 2, 4
EP = ("z", "y", "c")
F32, BF16 = jnp.float32, jnp.bfloat16
LIMIT = 16 << 20


def exchanged(x, axis):
    return lax.all_to_all(x, axis, split_axis=0, concat_axis=0, tiled=True)


def other_core(x):
    return lax.ppermute(x, "c", [(0, 1), (1, 0)])


def stacked_kernel(*refs):
    for i in range(NZ):
        refs[-1][i] = refs[i][...]


def gathered_z(x):
    pieces = [x] + [None] * (NZ - 1)
    up, down = x, x
    for s in range(1, NZ // 2 + 1):
        up = lax.ppermute(up, "z", [(i, (i + 1) % NZ) for i in range(NZ)])
        pieces[s] = up
        if s < NZ // 2:
            down = lax.ppermute(down, "z", [(i, (i - 1) % NZ) for i in range(NZ)])
            pieces[NZ - s] = down
    zs = pl.pallas_call(
        stacked_kernel,
        out_shape=jax.ShapeDtypeStruct((NZ, *x.shape), x.dtype),
        in_specs=[VMEM] * NZ,
        out_specs=VMEM,
        cost_estimate=pl.CostEstimate(flops=1 << 20, bytes_accessed=2 << 20, transcendentals=0),
        name="stacked",
    )(*pieces)
    return zs, other_core(zs)


def packed(x):
    h = x.shape[0] // 2
    return jnp.concatenate([x[:h], x[h:]], axis=1)


def turned_z(place_ref, z):
    az = lax.rem(place_ref[2] + (NZ - z), NZ)
    return pl.ds(pl.multiple_of(az * 128, 128), 128)


def both_kinds(c, r, n):
    lane = lax.broadcasted_iota(jnp.int32, (n, 128), 1)
    res = []
    for k in range(2):
        top, low = r[:n, k * 128 : (k + 1) * 128], r[n:, k * 128 : (k + 1) * 128]
        res.append((top + pltpu.roll(low, 64, 1), pltpu.roll(top, 64, 1) + low))
    first = jnp.where(c == 0, res[0][0], res[1][0])
    second = jnp.where(c == 0, res[1][1], res[0][1])
    return jnp.where(lane < 64, first, second)


def mix_kernel(c_ref, x0, x1, x2, x3, tok_ref, mine_ref, away_ref, out_ref):
    c = c_ref[0]
    xs = (x0, x1, x2, x3)
    both = jnp.concatenate([r[:16, :256] for r in xs] + [r[:16, 256:] for r in xs], axis=0)
    for z in range(NZ):
        w = jnp.concatenate([mine_ref[z, :256, :], away_ref[z, :256, :]], axis=1)
        tile = both_kinds(c, jnp.dot(both, w, preferred_element_type=F32), 64)
        tok = tok_ref[:, turned_z(c_ref, z)].astype(F32)
        for s in range(NY):
            to = lax.rem(c_ref[1] + (NY - s), NY)
            rows = tile[s * 16 : (s + 1) * 16] + jnp.where(to == c_ref[3], tok, 0.0)
            for x in range(NX):
                out_ref[to * NX + x, :, turned_z(c_ref, z)] = rows.astype(BF16)


VMEM = pl.BlockSpec(memory_space=pltpu.VMEM)
SMEM = pl.BlockSpec(memory_space=pltpu.SMEM)


def mix(c, heads, tok, mine, away):
    return pl.pallas_call(
        mix_kernel,
        out_shape=jax.ShapeDtypeStruct((NY * NX, 16, 1024), BF16),
        in_specs=[SMEM] + [VMEM] * 7,
        out_specs=VMEM,
        compiler_params=pltpu.CompilerParams(vmem_limit_bytes=LIMIT),
        cost_estimate=pl.CostEstimate(
            flops=2 * 128 * 256 * 128 * 16, bytes_accessed=2 << 20, transcendentals=0
        ),
        name="mix",
    )(c, *heads, tok, mine, away)


def settle_kernel(
    c_ref, got_ref, gain_ref, mix_ref, spread_ref,
    hid_ref, gate_ref, send_ref, n0_ref, n1_ref, n2_ref, n3_ref, norm_ref,
):
    square = jnp.zeros((16, 1), F32)
    dot = jnp.zeros((16, 1), F32)
    for y in range(NY):
        total = got_ref[y, 0].astype(F32)
        for x in range(1, NX):
            total += got_ref[y, x].astype(F32)
        for z in range(NZ):
            at = (z * NY + y) * 128
            cols = slice(at, at + 128)
            hid = total[:, z * 128 : (z + 1) * 128].astype(BF16)
            hid_ref[:, cols] = hid
            wide = hid.astype(F32)
            square += jnp.sum(wide * wide, axis=1, keepdims=True)
            dot += jnp.sum(wide * gain_ref[:, cols] * mix_ref[:, cols], axis=1, keepdims=True)
    inverse = lax.rsqrt(square / D + EPSILON)
    gate_ref[...] = jnp.broadcast_to(1.0 / (1.0 + jnp.exp(-(inverse * dot))), (16, 128))
    spread = spread_ref[...]
    for at in range(0, D, 512):
        cols = slice(at, at + 512)
        norm = (hid_ref[:, cols].astype(F32) * inverse * gain_ref[:, cols]).astype(BF16)
        norm_ref[:, cols] = norm
        rows = jnp.dot(spread, norm, preferred_element_type=F32)
        send_ref[:, :, cols] = rows.reshape(64, 2, 512).astype(BF16)
    for s, out in enumerate((n0_ref, n1_ref, n2_ref, n3_ref)):
        to = lax.rem(c_ref[1] + s, NY)
        for z in range(NZ):
            at = pl.multiple_of((z * NY + to) * 128, 128)
            out[:, z * 128 : (z + 1) * 128] = norm_ref[:, pl.ds(at, 128)]


def settle(c, got, gain, mix_row, spread):
    part = jax.ShapeDtypeStruct((16, 1024), BF16)
    return pl.pallas_call(
        settle_kernel,
        out_shape=(
            jax.ShapeDtypeStruct((16, D), BF16),
            jax.ShapeDtypeStruct((16, 128), F32),
            jax.ShapeDtypeStruct((64, 2, D), BF16),
            part, part, part, part,
        ),
        in_specs=[SMEM] + [VMEM] * 4,
        out_specs=(VMEM,) * 7,
        scratch_shapes=[pltpu.VMEM((16, D), BF16)],
        cost_estimate=pl.CostEstimate(
            flops=2 * 128 * 128 * 4096, bytes_accessed=3 << 20, transcendentals=0
        ),
        name="settle",
    )(c, got, gain, mix_row, spread)


def dense_kernel(c_ref, x0, x1, x2, x3, mine_ref, away_ref, out_ref):
    c = c_ref[0]
    acc = jnp.zeros((64, 512), F32)
    for z in range(NZ):
        cols = turned_z(c_ref, z)
        x = jnp.concatenate([r[:, cols] for r in (x0, x1, x2, x3)], axis=0)
        own = jnp.where(c == 0, x[:, :64], x[:, 64:])
        off = jnp.where(c == 0, x[:, 64:], x[:, :64])
        for part, ref in ((own, mine_ref), (off, away_ref)):
            w = jnp.concatenate(
                [ref[z, 272 + j * 64 : 336 + j * 64, :] for j in range(4)], axis=1
            )
            acc += jnp.dot(part, w, preferred_element_type=F32)
    out_ref[...] = acc.astype(BF16)


def dense_products(c, xs, mine, away):
    return pl.pallas_call(
        dense_kernel,
        out_shape=jax.ShapeDtypeStruct((64, 512), BF16),
        in_specs=[SMEM] + [VMEM] * 6,
        out_specs=VMEM,
        compiler_params=pltpu.CompilerParams(vmem_limit_bytes=LIMIT),
        cost_estimate=pl.CostEstimate(
            flops=2 * 64 * 1024 * 512, bytes_accessed=2 << 20, transcendentals=0
        ),
        name="dense_products",
    )(c, *xs, mine, away)


def dense_down_kernel(c_ref, x0, x1, x2, x3, mine_ref, away_ref, o0, o1, o2, o3):
    c = c_ref[0]
    xs = (x0, x1, x2, x3)
    units = []
    for s in range(NY):
        total = jnp.zeros((16, 512), F32)
        for k in range(NY):
            j = (s - k) % NY
            total += xs[k][j * 16 : (j + 1) * 16, :].astype(F32)
        gate = total[:, :256]
        units.append((gate / (1.0 + jnp.exp(-gate)) * total[:, 256:]).astype(BF16))
    both = jnp.concatenate([u[:, :128] for u in units] + [u[:, 128:] for u in units], axis=0)
    for z in range(NZ):
        w = jnp.concatenate([mine_ref[z, 528:656, :], away_ref[z, 528:656, :]], axis=1)
        tile = both_kinds(c, jnp.dot(both, w, preferred_element_type=F32), 64)
        for s, out in enumerate((o0, o1, o2, o3)):
            out[:, turned_z(c_ref, z)] = tile[s * 16 : (s + 1) * 16].astype(BF16)


def dense_down(c, xs, mine, away):
    part = jax.ShapeDtypeStruct((16, 1024), BF16)
    return pl.pallas_call(
        dense_down_kernel,
        out_shape=(part,) * 4,
        in_specs=[SMEM] + [VMEM] * 6,
        out_specs=(VMEM,) * 4,
        compiler_params=pltpu.CompilerParams(vmem_limit_bytes=LIMIT),
        cost_estimate=pl.CostEstimate(
            flops=2 * 64 * 1024 * 512, bytes_accessed=1 << 20, transcendentals=0
        ),
        name="dense_down",
    )(c, *xs, mine, away)


def half_rows(wide):
    lane = lax.broadcasted_iota(jnp.int32, (8, 128), 1)
    turn = pltpu.roll(wide, 64, 1)
    return (
        jnp.where(lane < 64, wide[:8], turn[8:]),
        jnp.where(lane < 64, turn[:8], wide[8:]),
    )


def down_kernel(c_ref, h_ref, w_ref, hid_ref, gate_ref, d0, d1, d2, d3, out_ref):
    res = jnp.dot(h_ref[...], w_ref[...], preferred_element_type=F32)
    lane = lax.broadcasted_iota(jnp.int32, (64, 128), 1)
    for p in range(8):
        cols = slice(p * 128, (p + 1) * 128)
        top, low = res[:64, cols], res[64:, cols]
        out_ref[2 * p, :64] = jnp.where(lane < 64, top, pltpu.roll(low, 64, 1)).astype(BF16)
        out_ref[2 * p + 1, :64] = jnp.where(lane < 64, pltpu.roll(top, 64, 1), low).astype(BF16)
    quarter = lax.broadcasted_iota(jnp.int32, (16, 128), 0) // 4 == c_ref[3]
    for zl in range(2):
        for s, d in enumerate((d0, d1, d2, d3)):
            at = zl * NY + lax.rem(c_ref[1] + s, NY)
            hid = hid_ref[:, pl.ds(pl.multiple_of(at * 128, 128), 128)].astype(F32)
            dense = d[:, zl * 128 : (zl + 1) * 128].astype(F32) * gate_ref[...]
            wide = dense + jnp.where(quarter, hid, 0.0)
            for k, half in enumerate(half_rows(wide)):
                out_ref[2 * at + k, 64:] = half.astype(BF16)


def down_for_all(c, expert_hidden, w, hidden, gate, downs):
    return pl.pallas_call(
        down_kernel,
        grid=(4,),
        out_shape=jax.ShapeDtypeStruct((64, 72, 128), BF16),
        in_specs=[
            SMEM,
            pl.BlockSpec((128, 256), lambda i: (0, 0)),
            pl.BlockSpec((256, 1024), lambda i: (0, i)),
            pl.BlockSpec((16, 1024), lambda i: (0, i)),
            pl.BlockSpec((16, 128), lambda i: (0, 0)),
        ]
        + [pl.BlockSpec((16, 256), lambda i: (0, i))] * 4,
        out_specs=pl.BlockSpec((16, 72, 128), lambda i: (i, 0, 0)),
        compiler_params=pltpu.CompilerParams(vmem_limit_bytes=LIMIT),
        cost_estimate=pl.CostEstimate(
            flops=2 * 128 * 256 * 4096, bytes_accessed=4 << 20, transcendentals=0
        ),
        name="down",
    )(c, expert_hidden, w, hidden, gate, *downs)


def project_kernel(kept, c_ref, tok_ref, gain_ref, q_ref, k_ref, v_ref, o_ref, i_ref, f_ref, *refs):
    got_ref, out, tile_ref, all_ref, x_ref = refs if kept else (None, refs[0], None, *refs[1:])
    c = c_ref[0]
    core = c if kept else 1 - c
    y = pl.program_id(0)

    @pl.when(y == 0)
    def _():
        all_ref[...] = jnp.transpose(tok_ref[...])

    gate_rows = jnp.concatenate(
        [jnp.zeros((64, 64), BF16), i_ref[...], f_ref[...], jnp.zeros((56, 64), BF16)], axis=0
    )
    for z in range(NZ):
        at = pl.multiple_of(((z * NY + y) * NC + core) * 16, 16)
        x_ref[z * 16 : (z + 1) * 16, :] = all_ref[pl.ds(at, 16), :]
    wide = x_ref[...].astype(F32)
    scaled = (wide * gain_ref[...].astype(F32)).astype(BF16)
    at = 0
    for w in (q_ref, k_ref, v_ref, o_ref):
        for half in range(0, w.shape[1], 256):
            res = jnp.dot(scaled, w[:, half : half + 256], preferred_element_type=F32)
            cols = slice(at, at + 256)
            if kept:
                res += got_ref[:, cols].astype(F32)
            out[0, :, cols] = res.astype(BF16)
            at += 256
    lane = lax.broadcasted_iota(jnp.int32, (128, 128), 1)
    gates = lax.dot_general(
        scaled, gate_rows, (((1,), (1,)), ((), ())), preferred_element_type=F32
    )
    square = jnp.sum(wide * wide, axis=1, keepdims=True)
    both = jnp.concatenate([wide, jnp.zeros((128, 64), F32)], axis=1)
    last = jnp.where(lane < 64, both, jnp.where(lane == 72, square, gates))
    if not kept:
        out[0, :, 1536:] = last.astype(BF16)
    else:
        other = got_ref[:, 1536:].astype(F32)
        out[0, :, 1536:1664] = (last + other).astype(BF16)

        @pl.when(y == c_ref[3])
        def _():
            first = jnp.where(c == 0, last, other)
            second = jnp.where(c == 0, other, last)
            tile_ref[...] = jnp.where(lane < 64, first, pltpu.roll(second, 64, 1)).astype(BF16)


def project(kept, *args):
    whole = lambda *shape: pl.BlockSpec(shape, lambda g: (0,) * len(shape))
    return pl.pallas_call(
        functools.partial(project_kernel, kept),
        grid=(NY,),
        out_shape=(jax.ShapeDtypeStruct((NY, 128, 1664), BF16),)
        + (jax.ShapeDtypeStruct((128, 128), BF16),) * kept,
        in_specs=[SMEM]
        + [whole(*a.shape) for a in args[1:9]]
        + [pl.BlockSpec((None, 128, 1664), lambda g: (g, 0, 0))] * kept,
        out_specs=(pl.BlockSpec((1, 128, 1664), lambda g: (g, 0, 0)),) + (whole(128, 128),) * kept,
        scratch_shapes=[pltpu.VMEM((1024, 64), BF16), pltpu.VMEM((128, 64), BF16)],
        cost_estimate=pl.CostEstimate(
            flops=2 * 512 * 256 * 1664, bytes_accessed=3 << 20, transcendentals=0
        ),
        name="project_kept" if kept else "project_away",
    )(*args)


def fold_y_kernel(in_ref, tile_ref, out_ref):
    for z in range(NZ):
        rows = slice(z * 16, (z + 1) * 16)
        total = in_ref[0, rows, :].astype(F32)
        for y in range(1, NY):
            total += in_ref[y, rows, :].astype(F32)
        out_ref[z, :, :1664] = total.astype(BF16)
        out_ref[z, :, 1664:] = tile_ref[rows, :]


def fold_y(x, tile):
    return pl.pallas_call(
        fold_y_kernel,
        out_shape=jax.ShapeDtypeStruct((NZ, 16, 1792), BF16),
        in_specs=[VMEM, VMEM],
        out_specs=VMEM,
        cost_estimate=pl.CostEstimate(
            flops=1 << 20, bytes_accessed=3 << 20, transcendentals=0
        ),
        name="fold_y",
    )(x, tile)


def recur_kernel(
    in_ref, ib_ref, fb_ref, hg_ref, sm_ref, sn_ref, mx_ref, ex_ref,
    heads_ref, tok_ref, nm_ref, nn_ref, nx_ref,
    kt_ref, qt_ref, car_ref, flo_ref, val_ref, out_ref, num_ref,
):
    g = pl.program_id(0)

    @pl.when(g == 0)
    def _():
        total = in_ref[0, :, :1664].astype(F32)
        for z in range(1, NZ):
            total += in_ref[z, :, :1664].astype(F32)
        for z in range(NZ):
            tok_ref[:, z * 128 : (z + 1) * 128] = in_ref[z, :, 1664:]
        inverse = lax.rsqrt(total[:, 1608:1609] / D + EPSILON)
        total = total * inverse
        q = total[:, :256].astype(BF16).astype(F32) * 0.125
        k = total[:, 256:512].astype(BF16).astype(F32)
        for h in range(4):
            cols = slice(512 + h * 128, 640 + h * 128)
            val_ref[h] = total[:, cols].astype(BF16).astype(F32)
        out_ref[...] = total[:, 1024:1536].astype(BF16).astype(F32)
        in_log = SOFT_CAP * jnp.tanh((total[:, 1600:1604] + ib_ref[...]) / SOFT_CAP)
        f = SOFT_CAP * jnp.tanh((total[:, 1604:1608] + fb_ref[...]) / SOFT_CAP)
        forget_log = jnp.minimum(f, 0.0) - jnp.log1p(jnp.exp(-jnp.abs(f)))
        kept = forget_log + mx_ref[...]
        top = jnp.maximum(kept, in_log)
        nx_ref[...] = top
        carried = jnp.exp(kept - top)
        fresh = jnp.exp(in_log - top)
        least = jnp.exp(-top)
        scaled = []
        for h in range(4):
            cols = slice(h * 64, (h + 1) * 64)
            fk = fresh[:, h : h + 1] * k[:, cols]
            scaled.append(fk)
            norm = carried[:, h : h + 1] * sn_ref[:, h, :] + fk
            nn_ref[:, h, :] = norm
            den = jnp.abs(jnp.sum(norm * q[:, cols], axis=1, keepdims=True))
            flo_ref[h] = jnp.broadcast_to(jnp.maximum(den, least[:, h : h + 1]), (16, 128))
            car_ref[h] = jnp.broadcast_to(carried[:, h : h + 1], (16, 128))
        kt = jnp.transpose(jnp.concatenate(scaled, axis=1))
        qt = jnp.transpose(q)
        for i in range(4):
            kt_ref[i] = kt[:, i * 4 : (i + 1) * 4]
            qt_ref[i] = qt[:, i * 4 : (i + 1) * 4]

    for i in range(4):
        b = g * 4 + i
        for h in range(4):
            rows = slice(h * 64, (h + 1) * 64)
            new = (
                car_ref[h, pl.ds(b, 1), :] * sm_ref[i, h]
                + kt_ref[g, rows, i : i + 1] * val_ref[h, pl.ds(b, 1), :]
            )
            nm_ref[i, h] = new
            num_ref[h, pl.ds(b, 1), :] = jnp.sum(
                new * qt_ref[g, rows, i : i + 1], axis=0, keepdims=True
            )

    @pl.when(g == 3)
    def _():
        heads_ref[16:, :] = ex_ref[...]
        for h in range(4):
            cols = slice(h * 128, (h + 1) * 128)
            read = num_ref[h] / flo_ref[h]
            mean = jnp.mean(read * read, axis=1, keepdims=True)
            gate = 1.0 / (1.0 + jnp.exp(-out_ref[:, cols]))
            scaled = read * lax.rsqrt(mean + EPSILON) * hg_ref[:, cols].astype(F32)
            heads_ref[:16, cols] = (scaled * gate).astype(BF16)


def recur(x, igate_bias, fgate_bias, head_gain, state_matrix, state_norm, state_max, extra):
    whole = lambda *shape: pl.BlockSpec(shape, lambda g: (0,) * len(shape))
    block = pl.BlockSpec((4, 4, 64, 128), lambda g: (g, 0, 0, 0))
    return pl.pallas_call(
        recur_kernel,
        grid=(4,),
        out_shape=(
            jax.ShapeDtypeStruct((24, 512), BF16),
            jax.ShapeDtypeStruct((16, 1024), BF16),
            jax.ShapeDtypeStruct((16, 4, 64, 128), F32),
            jax.ShapeDtypeStruct((16, 4, 64), F32),
            jax.ShapeDtypeStruct((16, 4), F32),
        ),
        in_specs=[
            whole(NZ, 16, 1792), whole(1, 4), whole(1, 4), whole(1, 512),
            block, whole(16, 4, 64), whole(16, 4), whole(8, 512),
        ],
        out_specs=(whole(24, 512), whole(16, 1024), block, whole(16, 4, 64), whole(16, 4)),
        scratch_shapes=[
            pltpu.VMEM((4, 256, 4), F32),
            pltpu.VMEM((4, 256, 4), F32),
            pltpu.VMEM((4, 16, 128), F32),
            pltpu.VMEM((4, 16, 128), F32),
            pltpu.VMEM((4, 16, 128), F32),
            pltpu.VMEM((16, 512), F32),
            pltpu.VMEM((4, 16, 128), F32),
        ],
        cost_estimate=pl.CostEstimate(
            flops=8 << 20, bytes_accessed=5 << 20, transcendentals=1 << 14
        ),
        name="recur",
    )(x, igate_bias[None], fgate_bias[None], head_gain[None], state_matrix, state_norm, state_max, extra)


def rank_kernel(me_ref, routes_ref, weights_ref, target_ref, spread_ref, weight_ref):
    me = me_ref[0]
    expert = lax.broadcasted_iota(jnp.int32, (64, 128), 0)
    a = lax.broadcasted_iota(jnp.int32, (128, 128), 0)
    b = lax.broadcasted_iota(jnp.int32, (128, 128), 1)
    before = jnp.where((a < b) & (a // 16 == b // 16), 1.0, 0.0).astype(BF16)
    weight = jnp.zeros((128, 128), F32)
    for t in range(8):
        cols = slice(t * 128, (t + 1) * 128)
        hits = [expert == routes_ref[j : j + 1, cols] for j in range(4)]
        count = sum(jnp.where(h, 1.0, 0.0) for h in hits)
        earlier = jnp.dot(count.astype(BF16), before, preferred_element_type=F32)
        for j in range(4):
            rank = jnp.sum(jnp.where(hits[j], earlier, 0.0), axis=0, keepdims=True)
            target = routes_ref[j : j + 1, cols] * 2 + rank.astype(jnp.int32)
            target_ref[j : j + 1, cols] = target
            mine = (target == me * 2 + a % 2) & (b // 16 + t * 8 == a // 2)
            weight += jnp.where(mine, weights_ref[j : j + 1, cols], 0.0)
    weight_ref[...] = jnp.broadcast_to(jnp.sum(weight, axis=1, keepdims=True), (128, 128))
    cols = pl.ds(pl.multiple_of((me // 8) * 128, 128), 128)
    named = a == target_ref[0:1, cols]
    for j in range(1, 4):
        named = named | (a == target_ref[j : j + 1, cols])
    lane = lax.broadcasted_iota(jnp.int32, (128, 16), 0)
    row = lax.broadcasted_iota(jnp.int32, (128, 16), 1)
    own = jnp.where(lane == lax.rem(me, 8) * 16 + row, 1.0, 0.0).astype(BF16)
    spread_ref[...] = jnp.dot(
        jnp.where(named, 1.0, 0.0).astype(BF16), own, preferred_element_type=F32
    ).astype(BF16)


def rank_rows(me, routes, weights):
    return pl.pallas_call(
        rank_kernel,
        out_shape=(
            jax.ShapeDtypeStruct((4, 1024), jnp.int32),
            jax.ShapeDtypeStruct((128, 16), BF16),
            jax.ShapeDtypeStruct((128, 128), F32),
        ),
        in_specs=[SMEM, VMEM, VMEM],
        out_specs=(VMEM,) * 3,
        cost_estimate=pl.CostEstimate(flops=1 << 24, bytes_accessed=1 << 20, transcendentals=0),
        name="rank_rows",
    )(me, routes, weights)


def pick_kernel(target_ref, out_ref):
    at = lax.broadcasted_iota(jnp.int32, (128, 128), 0)
    row = lax.broadcasted_iota(jnp.int32, (1, 128), 1)
    for t in range(8):
        cols = slice(t * 128, (t + 1) * 128)
        local = []
        for j in range(4):
            target = target_ref[j : j + 1, cols]
            local.append((target // 2) * 16 + 2 * (row // 16) + target % 2)
        for k in range(8):
            hit = at + k * 128 == local[0]
            for j in range(1, 4):
                hit = hit | (at + k * 128 == local[j])
            out_ref[t, k * 128 : (k + 1) * 128, :] = jnp.where(hit, 1.0, 0.0).astype(BF16)


def picks(target):
    return pl.pallas_call(
        pick_kernel,
        out_shape=jax.ShapeDtypeStruct((8, 1024, 128), BF16),
        in_specs=[VMEM],
        out_specs=VMEM,
        compiler_params=pltpu.CompilerParams(vmem_limit_bytes=LIMIT),
        cost_estimate=pl.CostEstimate(flops=1 << 24, bytes_accessed=2 << 20, transcendentals=0),
        name="picks",
    )(target)


def combine_kernel(got_ref, pick_ref, out_ref):
    lane = lax.broadcasted_iota(jnp.int32, (128, 128), 1)
    lane8 = lax.broadcasted_iota(jnp.int32, (8, 128), 1)
    for g in range(4):
        source = got_ref[:, g * 16 : (g + 1) * 16, :].reshape(1024, 128)
        first, second = (
            lax.dot_general(
                pick_ref[h * 4 + g], source, (((0,), (0,)), ((), ())), preferred_element_type=F32
            )
            for h in range(2)
        )
        rows = []
        for b in range(g * 8, g * 8 + 8):
            left = got_ref[b, 64:, :].astype(F32)
            right = got_ref[b + 32, 64:, :].astype(F32)
            rows.append(jnp.where(lane8 < 64, left, pltpu.roll(right, 64, 1)))
            rows.append(jnp.where(lane8 < 64, pltpu.roll(left, 64, 1), right))
        routed = jnp.where(lane < 64, first, second)
        out_ref[g * 128 : (g + 1) * 128, :] = (routed + jnp.concatenate(rows, axis=0)).astype(BF16)


def combine(returned, pick):
    return pl.pallas_call(
        combine_kernel,
        out_shape=jax.ShapeDtypeStruct((512, 128), BF16),
        in_specs=[VMEM, VMEM],
        out_specs=VMEM,
        compiler_params=pltpu.CompilerParams(vmem_limit_bytes=LIMIT),
        cost_estimate=pl.CostEstimate(flops=1 << 28, bytes_accessed=3 << 20, transcendentals=0),
        name="combine",
    )(returned, pick)


def finish_kernel(c_ref, b0, b1, b2, b3, out_ref):
    x = c_ref[3]
    parts = [r[...].astype(F32) for r in (b0, b1, b2, b3)]
    total = None
    for a in range(NX):
        s = lax.rem(x + (NX - a), NX)
        part = jnp.where(
            s == 0, parts[0], jnp.where(s == 1, parts[1], jnp.where(s == 2, parts[2], parts[3]))
        )
        total = part if total is None else total + part
    turned = jnp.transpose(total)
    out_ref[:, :512] = turned[:64].astype(BF16)
    out_ref[:, 512:] = turned[64:].astype(BF16)


def finish(c, parts):
    return pl.pallas_call(
        finish_kernel,
        out_shape=jax.ShapeDtypeStruct((64, 1024), BF16),
        in_specs=[SMEM] + [VMEM] * 4,
        out_specs=VMEM,
        compiler_params=pltpu.CompilerParams(vmem_limit_bytes=LIMIT),
        cost_estimate=pl.CostEstimate(flops=1 << 20, bytes_accessed=1 << 20, transcendentals=0),
        name="finish",
    )(c, *parts)


def layer(
    tokens,
    mix_gain,
    w_query,
    w_key,
    w_value,
    w_outgate,
    w_igate,
    w_fgate,
    igate_bias,
    fgate_bias,
    head_gain,
    w_mixout,
    state_matrix,
    state_norm,
    state_max,
    ffn_gain,
    dense_mix,
    w_dense_gate,
    w_dense_up,
    w_dense_down,
    routes,
    route_weights,
    w_exp_gate,
    w_exp_up,
    w_exp_down,
):
    me = lax.axis_index(EP)
    c = lax.axis_index("c")
    y, z = lax.axis_index("y"), lax.axis_index("z")
    c_ref = jnp.stack([c, y, z, lax.axis_index("x")]).astype(jnp.int32)
    piece = jnp.concatenate(
        [
            packed(w_mixout),
            jnp.stack([jnp.pad(ffn_gain, (0, 64)), jnp.pad(dense_mix, (0, 64))]),
            jnp.zeros((14, 128), BF16),
            w_dense_gate[:, :128],
            w_dense_gate[:, 128:],
            w_dense_up[:, :128],
            w_dense_up[:, 128:],
            packed(w_dense_down),
        ],
        axis=0,
    )
    operands = (
        c_ref, tokens.T, mix_gain[None], w_query, w_key, w_value, w_outgate, w_igate.T, w_fgate.T
    )
    (away,) = project(False, *operands)
    got = other_core(away)
    folded, tile = project(True, *operands, got)
    folded = exchanged(folded, "y")
    folded = fold_y(folded, tile)
    folded = exchanged(folded, "z")
    mine, away = gathered_z(piece)
    extra = jnp.stack([mine[:, 256:258, :64], away[:, 256:258, :64]])
    extra = jnp.where(c == 0, extra, extra[::-1])[:, (z - jnp.arange(NZ)) % NZ]
    extra = jnp.pad(extra.transpose(2, 1, 0, 3).reshape(4, 512), ((0, 4), (0, 0)))
    heads, tok, new_matrix, new_norm, new_max = recur(
        folded, igate_bias, fgate_bias, head_gain, state_matrix, state_norm, state_max, extra
    )
    heads = [heads] + [
        lax.ppermute(heads, "y", [(i, (i + s) % NY) for i in range(NY)]) for s in (1, 2, 3)
    ]
    vectors = jnp.stack([h[16:20] for h in heads])[(y - jnp.arange(NY)) % NY]
    vectors = vectors.reshape(NY, 2, NZ, 128).transpose(1, 2, 0, 3).reshape(2, 1, D)
    vectors = vectors.astype(F32)
    partial = mix(c_ref, heads, tok, mine, away)
    got = exchanged(partial, ("y", "x")).reshape(NY, NX, 16, 1024)
    target, spread, weight = rank_rows(
        jnp.full((1,), me, jnp.int32), routes.T, route_weights.T
    )
    hidden, dense_gate, send, *sides = settle(c_ref, got, vectors[0], vectors[1], spread)
    arrived = exchanged(send, EP).reshape(128, D)
    xs = [sides[0]] + [
        lax.ppermute(sides[s], "y", [(i, (i + s) % NY) for i in range(NY)]) for s in (1, 2, 3)
    ]
    sums = dense_products(c_ref, xs, mine, away)
    sums = [sums] + [
        lax.ppermute(sums, "y", [(i, (i + s) % NY) for i in range(NY)]) for s in (1, 2, 3)
    ]
    downs = dense_down(c_ref, sums, mine, away)
    downs = [downs[0]] + [
        lax.ppermute(downs[s], "y", [(i, (i - s) % NY) for i in range(NY)]) for s in (1, 2, 3)
    ]
    gate_part = jnp.dot(arrived, w_exp_gate[0], preferred_element_type=F32)
    up_part = jnp.dot(arrived, w_exp_up[0], preferred_element_type=F32)
    expert_hidden = (jax.nn.silu(gate_part) * up_part * weight[:, :1]).astype(BF16)
    returned = down_for_all(c_ref, expert_hidden, w_exp_down[0], hidden, dense_gate, downs)
    returned = exchanged(returned, EP)
    branch = combine(returned, picks(target))
    branches = [branch] + [
        lax.ppermute(branch, "x", [(i, (i + s) % NX) for i in range(NX)]) for s in (1, 2, 3)
    ]
    layer_out = finish(c_ref, branches).T
    return (layer_out, new_matrix, new_norm, new_max)


def solution(mesh):
    return jax.shard_map(
        layer,
        mesh=Mesh(mesh.devices.reshape(NZ, NY, NC, NX), ("z", "y", "c", "x")),
        in_specs=(
            P(None, EP),
            P(EP),
            P(EP, "x"),
            P(EP, "x"),
            P(EP, "x"),
            P(EP, "x"),
            P(EP, "x"),
            P(EP, "x"),
            P("x"),
            P("x"),
            P("x"),
            P("x", EP),
            P(EP, "x", None, None),
            P(EP, "x", None),
            P(EP, "x"),
            P(EP),
            P(EP),
            P(EP, "x"),
            P(EP, "x"),
            P("x", EP),
            P(),
            P(),
            P(EP, None, "x"),
            P(EP, None, "x"),
            P(EP, "x", None),
        ),
        out_specs=(P(None, EP), P(EP, "x", None, None), P(EP, "x", None), P(EP, "x")),
        check_vma=False,
    )
```
